32 devices in a mesh: ep: 16 (over z, x, core), tp: 2 (over y).
Axes of the slice: x: 2, y: 2, z: 4, core: 2. Of those that a mesh axis runs over, the one named last changes fastest.
Arguments:
- tokens: bfloat16 [256, 2048], P('ep'), may hold values from -6 to 6
- attn_gain: bfloat16 [2048], replicated, may hold values from 0.099609375 to 1.8984375
- query_weight: bfloat16 [2048, 1024], P('ep', 'tp'), may hold values from -0.125 to 0.125
- key_weight: bfloat16 [2048, 512], P('ep', 'tp'), may hold values from -0.125 to 0.125
- value_weight: bfloat16 [2048, 512], P('ep', 'tp'), may hold values from -0.125 to 0.125
- out_weight: bfloat16 [2048, 1024], P('ep', 'tp'), may hold values from -0.1875 to 0.1875
- head_gain: bfloat16 [1024], P('tp'), may hold values from 0.099609375 to 1.8984375
- past_keys: bfloat16 [256, 1024, 4, 128], P('ep', None, 'tp'), may hold values from -6 to 6
- past_values: bfloat16 [256, 1024, 4, 128], P('ep', None, 'tp'), may hold values from -50 to 50
- break_offset: float32 [256, 8, 1024], P('ep', 'tp'), may hold values from -12.5 to 1
- cache_lengths: int32 [256], P('ep'), may hold values from 1 to 1024, 131072 in all
- ffn_gain: bfloat16 [2048], replicated, may hold values from 0.099609375 to 1.8984375
- router_weight: bfloat16 [2048, 16], replicated, may hold values from -0.25 to 0.25
- expert_routes: int32 [256, 6], P('ep'), may hold values from 0 to 15, all different within a row; in each aligned block of 16 rows (0 to 15, 16 to 31, ...) at most 12 rows name the same one
- expert_gate: bfloat16 [16, 2048, 512], P('ep', None, 'tp'), may hold values from -0.125 to 0.125
- expert_up: bfloat16 [16, 2048, 512], P('ep', None, 'tp'), may hold values from -0.125 to 0.125
- expert_down: bfloat16 [16, 512, 2048], P('ep', 'tp'), may hold values from -0.25 to 0.25
- shared_gate: bfloat16 [2048, 512], P(None, 'tp'), may hold values from -0.125 to 0.125
- shared_up: bfloat16 [2048, 512], P(None, 'tp'), may hold values from -0.125 to 0.125
- shared_down: bfloat16 [512, 2048], P('tp'), may hold values from -0.25 to 0.25
Outputs:
- mixed: bfloat16 [256, 2048], P('ep', 'tp')
- fresh_keys: bfloat16 [256, 512], P('ep', 'tp')
- fresh_values: bfloat16 [256, 512], P('ep', 'tp')
The draws below stay inside these ranges and needn't reach their ends.
Inputs may be any that keep to these rules, and one draw needn't show every extreme that they name: `cache_lengths`: the lengths add up to half of 262144, and some sequence has length 1024. `expert_routes`: each row names 6 different experts. Among the rows of one device no expert is named more than 12 times, and 12 is reached in some device's rows.
All inputs are finite; a program needn't handle non-finite values. No bound on the sum of `cache_lengths` on one device may be relied on, other than what follows from the above.
Results may differ from the reference program's by a relative error of at most 0.0095.
Values may be sent and summed in bfloat16 or wider, within the bound.
No kernel may reach another device: no remote copies, remote signals or barrier semaphores. Data moves between devices by JAX's collectives and lax.ppermute only.
A program may use at most 64 MiB of HBM per device.

```python
import math
import jax
import jax.numpy as jnp
import numpy as np
from jax import lax

D = 2048
HQ = 8
KV = 4
HD = 128
EFF = 512
SFF = 512
TOP_K = 6
SEQ_DEV = 16
CACHE_POSITIONS = 1024
BATCH_SEQUENCES = 256
EXPERTS = 16
CAP = 12
N_EP = 16
N_TP = 2


def draw_break_offset(key, part):
    fast_share = 0.5
    quick_heads = jax.random.uniform(jax.random.fold_in(key, 101), (BATCH_SEQUENCES, HQ, 1)) < fast_share
    baseline_level = jnp.where(quick_heads, math.log(0.08), math.log(0.5 / CACHE_POSITIONS))
    slowdown_factor = jax.random.uniform(jax.random.fold_in(key, 102), (BATCH_SEQUENCES, HQ, 1), minval=0.0, maxval=math.log(3.0))
    jitter_amount = 0.7 * jnp.clip(jax.random.normal(jax.random.fold_in(key, 103), (BATCH_SEQUENCES, HQ, CACHE_POSITIONS)), -5.0, 5.0)
    spike_events = jax.random.uniform(jax.random.fold_in(key, 104), (BATCH_SEQUENCES, 1, CACHE_POSITIONS)) < 3.0 / CACHE_POSITIONS
    spike_level = jax.random.uniform(jax.random.fold_in(key, 105), (BATCH_SEQUENCES, 1, CACHE_POSITIONS), minval=-1.4, maxval=0.0)
    return jnp.where(spike_events, spike_level, baseline_level - slowdown_factor + jitter_amount).astype(jnp.float32)


def draw_past_values(key, part):
    values = jnp.clip(jax.random.normal(jax.random.fold_in(key, 201), (BATCH_SEQUENCES, CACHE_POSITIONS, KV, HD)), -5.0, 5.0)
    top_scale = 3.0
    head_ramp = jnp.arange(KV, dtype=jnp.float32) / max(KV - 1, 1)
    scales = top_scale ** head_ramp
    return (values * scales[None, None, :, None]).astype(jnp.bfloat16)


def block_levels(rng, extent, shards, low, high):
    loudness, own = 1.0, jax.random.fold_in(rng, 6)
    for position, shards_of in shards:
        draws = jnp.exp(jax.random.uniform(jax.random.fold_in(own, position), (shards_of,), jnp.float32, low / len(shards), high / len(shards)))
        loudness = loudness * jnp.repeat(draws, extent[position] // shards_of).reshape([-1 if axis == position else 1 for axis in range(len(extent))])
    return loudness


def length_profile(amount, total, limit, slope):
    portions = [(1 << 20) // math.isqrt(rank ** slope) + 1 for rank in range(2, amount + 1)]
    rest, counts = total - limit - (amount - 1), [1] * (amount - 1)
    while rest > 0:
        free = [i for i in range(amount - 1) if counts[i] < limit]
        pool, left = sum([portions[i] for i in free]), rest
        for i in free:
            more = min(limit - counts[i], max(1, left * portions[i] // pool), rest)
            counts[i] = counts[i] + more
            rest = rest - more
    return np.array([limit] + counts)


def ragged_sizes(own_key, count, total, reach, slope):
    if count == 2:
        one = jax.random.randint(own_key, (), max(1, total - reach), min(reach, total - 1) + 1)
        return jnp.stack([one, total - one])
    sizes = jnp.asarray(length_profile(count, total, reach, slope), jnp.int32)
    couples = (count - 1) // 2
    donor, receiver = sizes[1:1 + 2 * couples:2], sizes[2:2 + 2 * couples:2]
    room = jnp.minimum(donor - 1, reach - receiver)
    moved = jax.random.randint(jax.random.fold_in(own_key, 1), (couples,), 0, 1 << 20) % (room + 1)
    sizes = sizes.at[1:1 + 2 * couples:2].set(donor - moved).at[2:2 + 2 * couples:2].set(receiver + moved)
    return sizes[jax.random.permutation(jax.random.fold_in(own_key, 2), count)]


def routed_block(key, own, number, rows, count, top, most, skew):
    ranking = jax.random.permutation(key, count)
    packed, usual = load_shares(count, rows * top, most, skew, True), load_shares(count, rows * top, most, skew, False)
    places = jnp.arange(count)

    def named(tallies, rotation):
        used = int((tallies > 0).sum())
        fixed = max(1, used // 4)
        shifted = fixed + (places - fixed + rotation * (used - fixed)) % max(1, count - fixed)
        return jnp.zeros((count,), jnp.int32).at[ranking[jnp.where(places < fixed, places, shifted)]].set(jnp.asarray(tallies, jnp.int32))

    tallies = jnp.where(number % 4 == 0, named(packed, number // 4), named(usual, number - number // 4 - 1))
    mixed = jax.random.permutation(jax.random.fold_in(own, 3), count)
    source_of, taker = mixed[0:count // 2 * 2:2], mixed[1:count // 2 * 2:2]
    slack = jnp.minimum(tallies[source_of] - 1, most - tallies[taker]) // 2
    slack = jnp.where((source_of == ranking[0]) | (taker == ranking[0]) | (tallies[taker] == 0), 0, jnp.maximum(slack, 0))
    shifted = jax.random.randint(jax.random.fold_in(own, 4), (count // 2,), 0, 1 << 20) % (slack + 1)
    tallies = tallies.at[source_of].add(-shifted).at[taker].add(shifted)
    members = jnp.searchsorted(jnp.cumsum(tallies), jnp.arange(rows * top), side="right").astype(jnp.int32)
    grid = members.reshape(top, rows).T
    grid = grid[jax.random.permutation(jax.random.fold_in(own, 1), rows)]
    rotation = jax.random.randint(jax.random.fold_in(own, 2), (rows, 1), 0, top)
    return jnp.take_along_axis(grid, (jnp.arange(top)[None, :] + rotation) % top, axis=1)


def load_shares(number_of, total, bound, lean, full):
    loads = [(1 << 20) // math.isqrt(rank ** lean) + 1 for rank in range(1, number_of + 1)]
    largest = bound if full else min(bound, max(-(-total // number_of), total * loads[0] // sum(loads)))
    least = 1 if total - largest >= number_of - 1 else 0
    given, spare = [largest] + [least] * (number_of - 1), total - largest - least * (number_of - 1)
    while spare > 0:
        free = [i for i in range(1, number_of) if given[i] < largest] or [i for i in range(1, number_of) if given[i] < bound]
        whole, remaining = sum([loads[i] for i in free]), spare
        for i in free:
            addition = min(bound - given[i], max(1, remaining * loads[i] // whole), spare)
            given[i] = given[i] + addition
            spare = spare - addition
    return np.array(given)


def noise(own_key, dims, width, bound, cuts=(), kind=jnp.bfloat16):
    result = jax.random.normal(own_key, dims, jnp.float32) * width
    if len(cuts) > 0:
        result = block_levels(own_key, dims, cuts, -0.22, 0.18) * result
    return jnp.clip(result, min=-bound, max=bound).astype(kind)


def setup_inputs(seed: int = 0) -> dict:
    arg_keys = jax.random.split(jax.random.key(seed), 21)
    tokens = noise(arg_keys[0], (BATCH_SEQUENCES, D), 1.0, 6.0, ((0, 16),))
    attn_gain = jnp.clip(1.0 + 0.18 * jax.random.normal(arg_keys[1], (D,), jnp.float32), 0.099609375, 1.8984375).astype(jnp.bfloat16)
    query_weight = noise(arg_keys[2], (D, HQ * HD), D ** -0.5, 0.125, ((0, 16), (1, 2)))
    key_weight = noise(arg_keys[3], (D, KV * HD), D ** -0.5, 0.125, ((0, 16), (1, 2)))
    value_weight = noise(arg_keys[4], (D, KV * HD), D ** -0.5, 0.125, ((0, 16), (1, 2)))
    out_weight = noise(arg_keys[5], (D, HQ * HD), (HQ * HD) ** -0.5, 0.1875, ((0, 16), (1, 2)))
    head_gain = jnp.clip(1.0 + 0.18 * jax.random.normal(arg_keys[6], (HQ * HD,), jnp.float32), 0.099609375, 1.8984375).astype(jnp.bfloat16)
    past_keys = noise(arg_keys[7], (BATCH_SEQUENCES, CACHE_POSITIONS, KV, HD), 1.0, 6.0, ((0, 16), (2, 2)))
    past_values = draw_past_values(jax.random.fold_in(arg_keys[20], 71), 0)
    break_offset = draw_break_offset(jax.random.fold_in(arg_keys[20], 71), 0)
    cache_lengths = ragged_sizes(arg_keys[10], BATCH_SEQUENCES, BATCH_SEQUENCES * CACHE_POSITIONS // 2, CACHE_POSITIONS, 2).astype(jnp.int32)
    ffn_gain = jnp.clip(1.0 + 0.18 * jax.random.normal(arg_keys[11], (D,), jnp.float32), 0.099609375, 1.8984375).astype(jnp.bfloat16)
    router_weight = noise(arg_keys[12], (D, EXPERTS), (D // 4) ** -0.5, 0.25)
    expert_routes_keys = jax.random.split(jax.random.fold_in(arg_keys[13], 1), BATCH_SEQUENCES // SEQ_DEV)
    expert_routes_turns = jax.random.permutation(jax.random.fold_in(arg_keys[13], 3), BATCH_SEQUENCES // SEQ_DEV)
    expert_routes = jax.vmap(lambda own, number: routed_block(jax.random.fold_in(arg_keys[13], 2), own, number, SEQ_DEV, EXPERTS, TOP_K, CAP, 2))(expert_routes_keys, expert_routes_turns).reshape((BATCH_SEQUENCES, TOP_K))
    expert_gate = noise(arg_keys[14], (EXPERTS, D, EFF), D ** -0.5, 0.125, ((0, 16), (2, 2)))
    expert_up = noise(arg_keys[15], (EXPERTS, D, EFF), D ** -0.5, 0.125, ((0, 16), (2, 2)))
    expert_down = noise(arg_keys[16], (EXPERTS, EFF, D), EFF ** -0.5, 0.25, ((0, 16), (1, 2)))
    shared_gate = noise(arg_keys[17], (D, SFF), D ** -0.5, 0.125, ((1, 2),))
    shared_up = noise(arg_keys[18], (D, SFF), D ** -0.5, 0.125, ((1, 2),))
    shared_down = noise(arg_keys[19], (SFF, D), SFF ** -0.5, 0.25, ((0, 2),))
    return {"tokens": tokens, "attn_gain": attn_gain, "query_weight": query_weight, "key_weight": key_weight, "value_weight": value_weight, "out_weight": out_weight, "head_gain": head_gain, "past_keys": past_keys, "past_values": past_values, "break_offset": break_offset, "cache_lengths": cache_lengths, "ffn_gain": ffn_gain, "router_weight": router_weight, "expert_routes": expert_routes, "expert_gate": expert_gate, "expert_up": expert_up, "expert_down": expert_down, "shared_gate": shared_gate, "shared_up": shared_up, "shared_down": shared_down}


epsilon = 1e-06
routed_scale = 2.5

def root_norm(values, gain):
    data = values.astype(jnp.float32)
    factor = lax.rsqrt(lax.optimization_barrier(jnp.mean(data * data, axis=-1, keepdims=True)) + epsilon)
    return (data * factor * gain.astype(jnp.float32)).astype(jnp.bfloat16)

def rounded(values):
    return lax.optimization_barrier(values.astype(jnp.bfloat16)).astype(jnp.float32)

def group_sum(left_side, right_side, groups):
    width_part = left_side.shape[1] // groups
    running = jnp.zeros((left_side.shape[0], right_side.shape[1]), jnp.float32)
    for group_index in range(groups):
        piece_left = left_side[:, group_index * width_part:(group_index + 1) * width_part]
        piece_right = right_side[group_index * width_part:(group_index + 1) * width_part]
        running = running + rounded(jnp.dot(piece_left, piece_right, preferred_element_type=jnp.float32))
    return running

def reference(tokens, attn_gain, query_weight, key_weight, value_weight, out_weight, head_gain, past_keys, past_values, break_offset, cache_lengths, ffn_gain, router_weight, expert_routes, expert_gate, expert_up, expert_down, shared_gate, shared_up, shared_down):
    normed = root_norm(tokens, attn_gain)
    queries = jnp.dot(normed, query_weight, preferred_element_type=jnp.float32).astype(jnp.bfloat16)
    fresh_keys = jnp.dot(normed, key_weight, preferred_element_type=jnp.float32).astype(jnp.bfloat16)
    fresh_values = jnp.dot(normed, value_weight, preferred_element_type=jnp.float32).astype(jnp.bfloat16)
    group_size = HQ // KV

    def attend(inputs):
        block_queries, block_keys, block_values, block_offsets, block_lengths = inputs
        grouped = block_queries.astype(jnp.float32).reshape(SEQ_DEV, KV, group_size, HD)
        scores = jnp.einsum('bgrd,blgd->bgrl', grouped, block_keys.astype(jnp.float32))
        logits = scores.reshape(SEQ_DEV, HQ, CACHE_POSITIONS) * HD ** (-0.5) + block_offsets
        places = jnp.arange(CACHE_POSITIONS, dtype=jnp.int32)[None, None, :]
        usable = places < block_lengths[:, None, None]
        keep_log = jnp.where(usable, jax.nn.log_sigmoid(-logits), 0.0)
        after_sum = lax.cumsum(keep_log, axis=2, reverse=True) - keep_log
        sticks = jnp.where(usable, jnp.exp(jax.nn.log_sigmoid(logits) + after_sum), 0.0)
        sticks = rounded(sticks).reshape(SEQ_DEV, KV, group_size, CACHE_POSITIONS)
        outputs = jnp.einsum('bgrl,blgd->bgrd', sticks, block_values.astype(jnp.float32))
        return outputs.reshape(SEQ_DEV, HQ * HD)
    heads_out = lax.map(attend, (queries.reshape(N_EP, SEQ_DEV, HQ * HD), past_keys.reshape(N_EP, SEQ_DEV, CACHE_POSITIONS, KV, HD), past_values.reshape(N_EP, SEQ_DEV, CACHE_POSITIONS, KV, HD), break_offset.reshape(N_EP, SEQ_DEV, HQ, CACHE_POSITIONS), cache_lengths.reshape(N_EP, SEQ_DEV))).reshape(BATCH_SEQUENCES, HQ * HD)
    scaled = (heads_out * head_gain.astype(jnp.float32)).astype(jnp.bfloat16)
    square_sum = lax.optimization_barrier(jnp.sum(heads_out * heads_out, axis=-1))
    head_total = group_sum(scaled, out_weight.T, N_TP)
    attention = head_total * lax.rsqrt(square_sum[:, None] / (HQ * HD) + epsilon)
    residual = (tokens.astype(jnp.float32) + attention).astype(jnp.bfloat16)
    normed_ffn = root_norm(residual, ffn_gain)
    router_prob = jax.nn.sigmoid(jnp.dot(normed_ffn, router_weight, preferred_element_type=jnp.float32))
    picked = jnp.take_along_axis(router_prob, expert_routes, axis=1)
    route_weight = routed_scale * picked / lax.optimization_barrier(jnp.sum(picked, axis=-1, keepdims=True))
    flat_routes = expert_routes.reshape(N_EP, SEQ_DEV * TOP_K)
    flat_hot = (flat_routes[:, :, None] == jnp.arange(EXPERTS, dtype=jnp.int32)[None, None, :]).astype(jnp.int32)
    earlier = jnp.cumsum(flat_hot, axis=1) - flat_hot
    slot_index = lax.optimization_barrier(jnp.sum(earlier * flat_hot, axis=-1)).astype(jnp.int32)
    owner_group = jnp.broadcast_to(jnp.arange(N_EP, dtype=jnp.int32)[:, None], flat_routes.shape)
    pair_row = jnp.broadcast_to((jnp.arange(SEQ_DEV * TOP_K, dtype=jnp.int32) // TOP_K)[None, :], flat_routes.shape)
    row_number = (owner_group * SEQ_DEV + pair_row).astype(jnp.int32)
    row_table = jnp.full((EXPERTS, N_EP, CAP), BATCH_SEQUENCES, jnp.int32).at[flat_routes, owner_group, slot_index].set(row_number)
    padded_rows = jnp.concatenate([normed_ffn, jnp.zeros((1, D), jnp.bfloat16)], axis=0)

    def one_expert(inputs):
        row_ids, gate_matrix, up_matrix, down_matrix = inputs
        chosen_rows = padded_rows[row_ids.reshape(-1)]
        gate_part = jnp.dot(chosen_rows, gate_matrix, preferred_element_type=jnp.float32)
        up_part = jnp.dot(chosen_rows, up_matrix, preferred_element_type=jnp.float32)
        hidden = (jax.nn.silu(gate_part) * up_part).astype(jnp.bfloat16)
        return group_sum(hidden, down_matrix, N_TP).astype(jnp.bfloat16)
    expert_out = lax.map(one_expert, (row_table, expert_gate, expert_up, expert_down))
    taken = expert_out[flat_routes, (owner_group * CAP + slot_index).astype(jnp.int32)]
    taken = taken.reshape(BATCH_SEQUENCES, TOP_K, D).astype(jnp.float32)
    routed = lax.optimization_barrier(jnp.sum(route_weight[:, :, None] * taken, axis=1))
    shared_hidden = (jax.nn.silu(jnp.dot(normed_ffn, shared_gate, preferred_element_type=jnp.float32)) * jnp.dot(normed_ffn, shared_up, preferred_element_type=jnp.float32)).astype(jnp.bfloat16)
    shared_out = group_sum(shared_hidden, shared_down, N_TP)
    mixed = (residual.astype(jnp.float32) + routed + shared_out).astype(jnp.bfloat16)
    return (mixed, fresh_keys, fresh_values)
```

```python
import jax
import jax.numpy as jnp
from jax import lax
from jax.experimental import pallas as pl
from jax.experimental.pallas import tpu as pltpu
from jax.sharding import PartitionSpec as P


epsilon = 1e-06
routed_scale = 2.5
LANES = 128
bf16 = jnp.bfloat16
f32 = jnp.float32


def dot(a, b, dims=((1,), (0,)), precision=None):
    return lax.dot_general(a, b, (dims, ((), ())), precision=precision, preferred_element_type=f32)


def split3(value):
    high = value.astype(bf16)
    rest = value - high.astype(f32)
    mid = rest.astype(bf16)
    low = (rest - mid.astype(f32)).astype(bf16)
    return high, mid, low


def attend_kernel(lengths, q_ref, k_ref, v_ref, off_ref, gain_ref, out_ref, heads_ref, *, seqs, heads, key_heads):
    step = pl.program_id(0)
    rows2 = k_ref.shape[1]
    head_size = k_ref.shape[2]
    half = rows2 // 2
    positions = rows2 // key_heads
    block = LANES * key_heads
    group = heads // key_heads
    both = 2 * heads
    row = lax.broadcasted_iota(jnp.int32, (both, half), 0)
    col = lax.broadcasted_iota(jnp.int32, (both, half), 1)
    place = jnp.where(row >= heads, positions // 2, 0) + col // key_heads
    mine = (col % key_heads) == ((row % heads) // group)
    low_row = row < heads
    spread = (
        lax.broadcasted_iota(jnp.int32, (LANES, block), 1) // key_heads
        == lax.broadcasted_iota(jnp.int32, (LANES, block), 0)
    ).astype(f32)
    tri_row = lax.broadcasted_iota(jnp.int32, (LANES, 2 * LANES), 0)
    tri_col = lax.broadcasted_iota(jnp.int32, (LANES, 2 * LANES), 1)
    tri = ((tri_row > tri_col) | (tri_col >= LANES)).astype(f32)
    scale = head_size ** (-0.5)
    blocks = half // LANES
    for s in range(seqs):
        q8 = q_ref[s]
        s_lo = dot(q8, k_ref[s, :half, :], ((1,), (1,)))
        s_hi = dot(q8, k_ref[s, half:, :], ((1,), (1,)))
        off = off_ref[s]
        off8 = jnp.concatenate([off[:, : positions // 2], off[:, positions // 2 :]], axis=0)
        stacked = jnp.concatenate(
            [off8[:, b * LANES : (b + 1) * LANES] for b in range(positions // 2 // LANES)], axis=0
        )
        wide = dot(stacked, spread, precision=lax.Precision.HIGHEST)
        off_wide = jnp.concatenate(
            [wide[b * both : (b + 1) * both] for b in range(positions // 2 // LANES)], axis=1
        )
        logits = jnp.where(low_row, s_lo, s_hi) * scale + off_wide
        valid = mine & (place < lengths[step * seqs + s])
        tail = jnp.log1p(jnp.exp(-jnp.abs(logits)))
        log_stop = jnp.minimum(logits, 0.0) - tail
        keep = jnp.where(valid, -jnp.maximum(logits, 0.0) - tail, 0.0)
        keep_rows = jnp.concatenate([keep[:, b * LANES : (b + 1) * LANES] for b in range(blocks)], axis=0)
        sums = dot(keep_rows, tri, precision=lax.Precision.HIGHEST)
        after = [None] * blocks
        running = jnp.zeros((both, LANES), f32)
        for b in reversed(range(blocks)):
            after[b] = sums[b * both : (b + 1) * both, :LANES] + running
            running = running + sums[b * both : (b + 1) * both, LANES:]
        upper = pltpu.roll(running, heads, 0)
        upper = jnp.where(lax.broadcasted_iota(jnp.int32, (both, LANES), 0) < heads, upper, 0.0)
        after_sum = jnp.concatenate([a + upper for a in after], axis=1)
        sticks = jnp.where(valid, jnp.exp(log_stop + after_sum), 0.0).astype(bf16)
        o_lo = dot(sticks, v_ref[s, :half, :])
        o_hi = dot(sticks, v_ref[s, half:, :])
        out = o_lo + pltpu.roll(o_hi, heads, 0)
        for h in range(heads):
            heads_ref[step, s : s + 1, h * head_size : (h + 1) * head_size] = out[h : h + 1]

    @pl.when(step == pl.num_programs(0) - 1)
    def _():
        values = jnp.concatenate([heads_ref[i] for i in range(heads_ref.shape[0])], axis=0)
        width = values.shape[1]
        out_ref[:, :width] = (values * gain_ref[...].astype(f32)).astype(bf16)
        square = jnp.sum(values * values, axis=1, keepdims=True)
        high, mid, low = [p.astype(f32) for p in split3(square)]
        lane = lax.broadcasted_iota(jnp.int32, (values.shape[0], LANES), 1)
        extra = jnp.where(lane == 0, high, jnp.where(lane == 1, mid, jnp.where(lane == 2, low, 0.0)))
        out_ref[:, width:] = extra.astype(bf16)


def attend(queries, key_cache, value_cache, offsets, lengths, head_gain):
    seq_count, positions, key_heads, head_size = key_cache.shape
    heads = offsets.shape[1]
    seqs = 4
    rows = positions * key_heads
    keys = key_cache.reshape(seq_count, rows, head_size)
    values = value_cache.reshape(seq_count, rows, head_size)
    grouped = queries.reshape(seq_count, heads, head_size)
    doubled = jnp.concatenate([grouped, grouped], axis=1)
    width = heads * head_size

    def kernel(*refs):
        attend_kernel(*refs, seqs=seqs, heads=heads, key_heads=key_heads)

    return pl.pallas_call(
        kernel,
        out_shape=jax.ShapeDtypeStruct((seq_count, width + LANES), bf16),
        grid_spec=pltpu.PrefetchScalarGridSpec(
            num_scalar_prefetch=1,
            grid=(seq_count // seqs,),
            in_specs=[
                pl.BlockSpec((seqs, 2 * heads, head_size), lambda i, n: (i, 0, 0)),
                pl.BlockSpec((seqs, rows, head_size), lambda i, n: (i, 0, 0)),
                pl.BlockSpec((seqs, rows, head_size), lambda i, n: (i, 0, 0)),
                pl.BlockSpec((seqs, heads, positions), lambda i, n: (i, 0, 0)),
                pl.BlockSpec((1, width), lambda i, n: (0, 0)),
            ],
            out_specs=pl.BlockSpec((seq_count, width + LANES), lambda i, n: (0, 0)),
            scratch_shapes=[pltpu.VMEM((seq_count // seqs, seqs, width), f32)],
        ),
        compiler_params=pltpu.CompilerParams(dimension_semantics=("arbitrary",)),
        name="stick_attend",
    )(lengths, doubled, keys, values, offsets, head_gain.reshape(1, width))


def make_body(n_ep, n_tp):
    inner = 1 << ((n_ep.bit_length() - 1) // 2)
    outer = n_ep // inner

    def swap(value, mask):
        return lax.ppermute(value, "ep", [(i, i ^ mask) for i in range(n_ep)])

    def outer_swap(value, k):
        return swap(value, k * inner)

    def tp_swap(value):
        return lax.ppermute(value, "tp", [(i, (i + 1) % n_tp) for i in range(n_tp)])

    def inner_masks():
        masks, m = [], inner // 2
        while m >= 1:
            masks.append(m)
            m //= 2
        return masks

    def inner_gather(value):
        order = [0]
        parts = value
        for m in inner_masks():
            parts = jnp.concatenate([parts, swap(parts, m)], axis=0)
            order = order + [o ^ m for o in order]
        return parts, order

    def body(
        tokens,
        attn_gain,
        query_weight,
        key_weight,
        value_weight,
        out_weight,
        head_gain,
        past_keys,
        past_values,
        break_offset,
        cache_lengths,
        ffn_gain,
        router_weight,
        expert_routes,
        expert_gate,
        expert_up,
        expert_down,
        shared_gate,
        shared_up,
        shared_down,
    ):
        seqs, model = tokens.shape
        experts = router_weight.shape[1]
        block = query_weight.shape[0]
        plane = block * inner
        query_cols = query_weight.shape[1]
        key_cols = key_weight.shape[1]
        pad = -experts % LANES
        me = lax.axis_index("ep")
        my_inner = me % inner
        my_outer = me // inner
        my_tp = lax.axis_index("tp")

        lane = lax.broadcasted_iota(jnp.int32, (1, 1, experts + pad), 2)
        routed_mask = jnp.sum((expert_routes[:, :, None] == lane).astype(f32), axis=1).astype(bf16)

        planes = tokens.reshape(seqs, outer, plane)

        def plane_of(index):
            return lax.dynamic_slice_in_dim(planes, index, 1, 1)[:, 0]

        joined = jnp.concatenate([query_weight, key_weight, value_weight], axis=1)
        with jax.named_scope("token_exchange"):
            message = [jnp.concatenate([plane_of(my_outer ^ k), routed_mask], axis=1) for k in range(outer)]
            got = [message[0]] + [outer_swap(message[k], k) for k in range(1, outer)]
        with jax.named_scope("weights"):
            wide_weight, order = inner_gather(joined)
            wide_out, _ = inner_gather(out_weight)
        arrived = jnp.concatenate(got, axis=0)
        group_tokens = arrived[:, :plane]
        group_mask = arrived[:, plane:]

        def by_order(value):
            pieces = value.reshape(value.shape[0], inner, block)
            return jnp.concatenate(
                [lax.dynamic_slice_in_dim(pieces, my_inner ^ o, 1, 1)[:, 0] for o in order], axis=1
            )

        gain_plane = lax.dynamic_slice_in_dim(attn_gain, my_outer * plane, plane, 0)
        gained = (group_tokens.astype(f32) * gain_plane.astype(f32)).astype(bf16)
        partial = dot(by_order(gained), wide_weight).astype(bf16)
        partial = partial.reshape(outer, seqs, -1)
        with jax.named_scope("product_exchange"):
            total = partial[0].astype(f32)
            for k in range(1, outer):
                total = total + outer_swap(partial[k], k).astype(f32)
        wide_tokens = tokens.astype(f32)
        factor = lax.rsqrt(jnp.mean(wide_tokens * wide_tokens, axis=-1, keepdims=True) + epsilon)
        projected = (total * factor).astype(bf16)
        queries = projected[:, :query_cols]
        fresh_keys = projected[:, query_cols : query_cols + key_cols]
        fresh_values = projected[:, query_cols + key_cols :]

        with jax.named_scope("mask_exchange"):
            all_mask, _ = inner_gather(group_mask)

        scaled = attend(queries, past_keys, past_values, break_offset, cache_lengths, head_gain)
        with jax.named_scope("scaled_gather"):
            group_scaled = jnp.concatenate([scaled] + [outer_swap(scaled, k) for k in range(1, outer)], axis=0)
        heads_width = out_weight.shape[1]
        out_part = dot(group_scaled[:, :heads_width], wide_out, ((1,), (1,))).astype(bf16)
        own_part = jnp.concatenate([out_part, group_scaled[:, heads_width:]], axis=1)
        with jax.named_scope("head_swap"):
            other_part = tp_swap(own_part)
        both = own_part.astype(f32) + other_part.astype(f32)
        square_total = jnp.sum(both[:, plane:], axis=1, keepdims=True)
        attention = both[:, :plane] * lax.rsqrt(square_total / (heads_width * n_tp) + epsilon)
        residual_part = (by_order(group_tokens).astype(f32) + attention).astype(bf16)

        pieces = residual_part.reshape(outer * seqs, inner, block)
        position = {o: i for i, o in enumerate(order)}
        table = jnp.array([position[o] for o in range(inner)], jnp.int32)
        residual_plane = jnp.concatenate(
            [
                lax.dynamic_slice_in_dim(pieces, table[my_inner ^ o], 1, 1)[:, 0]
                for o in range(inner)
            ],
            axis=1,
        )
        with jax.named_scope("row_gather"):
            blocks = [residual_plane] + [outer_swap(residual_plane, k) for k in range(1, outer)]
            rows = []
            for k in range(outer):
                peer = blocks[k].reshape(outer, seqs, plane)
                rows.append(jnp.stack([peer[j ^ k] for j in range(outer)], axis=0))
            stacked = jnp.stack(rows, axis=0)
            group_rows = jnp.concatenate(
                [
                    lax.dynamic_slice_in_dim(stacked, my_outer ^ p, 1, 0)[0].reshape(outer * seqs, plane)
                    for p in range(outer)
                ],
                axis=1,
            )
            all_rows, _ = inner_gather(group_rows)

        def normalize(value):
            data = value.astype(f32)
            scale = lax.rsqrt(jnp.mean(data * data, axis=-1, keepdims=True) + epsilon)
            return (data * scale * ffn_gain.astype(f32)).astype(bf16)

        own_rows = group_rows[:seqs]
        own_normed = normalize(own_rows)
        shared_hidden = (
            jax.nn.silu(dot(own_normed, shared_gate)) * dot(own_normed, shared_up)
        ).astype(bf16)
        shared_part = dot(shared_hidden, shared_down)

        normed = normalize(all_rows)
        prob = jax.nn.sigmoid(dot(normed, router_weight)) * all_mask[:, :experts].astype(f32)
        weight = routed_scale * prob / jnp.sum(prob, axis=-1, keepdims=True)
        local = expert_gate.shape[0]
        combined = None
        for e in range(local):
            hidden = (
                jax.nn.silu(dot(normed, expert_gate[e])) * dot(normed, expert_up[e])
            ).astype(bf16)
            mine = lax.dynamic_slice_in_dim(weight, me * local + e, 1, 1)
            piece = dot(hidden, expert_down[e]) * mine
            combined = piece if combined is None else combined + piece
        combined = combined.astype(bf16)

        with jax.named_scope("combine"):
            value = combined
            for m in reversed(inner_masks()):
                count = value.shape[0] // 2
                value = (value[:count].astype(f32) + swap(value[count:], m).astype(f32)).astype(bf16)
            value = jnp.concatenate([(value[:seqs].astype(f32) + shared_part).astype(bf16), value[seqs:]], axis=0)
            cols = model // n_tp
            halves = value.reshape(outer * seqs, n_tp, cols)
            keep = lax.dynamic_slice_in_dim(halves, my_tp, 1, 1)[:, 0]
            send = lax.dynamic_slice_in_dim(halves, (my_tp + 1) % n_tp, 1, 1)[:, 0]
            value = (keep.astype(f32) + tp_swap(send).astype(f32)).astype(bf16).reshape(outer, seqs, cols)
            total = value[0].astype(f32)
            for k in range(1, outer):
                total = total + outer_swap(value[k], k).astype(f32)
        own_cols = lax.dynamic_slice_in_dim(own_rows, my_tp * cols, cols, 1)
        mixed = (own_cols.astype(f32) + total).astype(bf16)
        return mixed, fresh_keys, fresh_values

    return body


def solution(mesh):
    placed = (
        P("ep", None),
        P(),
        P("ep", "tp"),
        P("ep", "tp"),
        P("ep", "tp"),
        P("ep", "tp"),
        P("tp"),
        P("ep", None, "tp", None),
        P("ep", None, "tp", None),
        P("ep", "tp", None),
        P("ep"),
        P(),
        P(),
        P("ep", None),
        P("ep", None, "tp"),
        P("ep", None, "tp"),
        P("ep", "tp", None),
        P(None, "tp"),
        P(None, "tp"),
        P("tp", None),
    )
    return jax.shard_map(
        make_body(mesh.shape["ep"], mesh.shape["tp"]),
        mesh=mesh,
        in_specs=placed,
        out_specs=(P("ep", "tp"), P("ep", "tp"), P("ep", "tp")),
        check_vma=False,
    )
```

```python
import jax
import jax.numpy as jnp
from jax import lax
from jax.experimental import pallas as pl
from jax.experimental.pallas import tpu as pltpu
from jax.sharding import PartitionSpec as P


epsilon = 1e-06
routed_scale = 2.5
LANES = 128
bf16 = jnp.bfloat16
f32 = jnp.float32


def dot(a, b, dims=((1,), (0,)), precision=None):
    return lax.dot_general(a, b, (dims, ((), ())), precision=precision, preferred_element_type=f32)


def split3(value):
    high = value.astype(bf16)
    rest = value - high.astype(f32)
    mid = rest.astype(bf16)
    low = (rest - mid.astype(f32)).astype(bf16)
    return high, mid, low


def split2(value):
    high = value.astype(bf16)
    return high, (value - high.astype(f32)).astype(bf16)


def attend_kernel(lengths, q_ref, k_ref, v_ref, off_ref, gain_ref, out_ref, heads_ref, *, seqs, heads, key_heads):
    step = pl.program_id(0)
    rows = k_ref.shape[1]
    head_size = k_ref.shape[2]
    half = rows // 2
    positions = rows // key_heads
    block = LANES * key_heads
    group = heads // key_heads
    both = 2 * heads
    blocks = half // LANES
    off_blocks = positions // 2 // LANES
    row = lax.broadcasted_iota(jnp.int32, (both, half), 0)
    col = lax.broadcasted_iota(jnp.int32, (both, half), 1)
    place = jnp.where(row >= heads, positions // 2, 0) + col // key_heads
    mine = (col % key_heads) == ((row % heads) // group)
    low_row = row < heads
    scale = head_size ** (-0.5)
    spread = (
        lax.broadcasted_iota(jnp.int32, (LANES, block), 1) // key_heads
        == lax.broadcasted_iota(jnp.int32, (LANES, block), 0)
    ).astype(bf16)
    tri_row = lax.broadcasted_iota(jnp.int32, (LANES, 2 * LANES), 0)
    tri_col = lax.broadcasted_iota(jnp.int32, (LANES, 2 * LANES), 1)
    tri = ((tri_row > tri_col) | (tri_col >= LANES)).astype(bf16)

    scores = []
    for s in range(seqs):
        own = q_ref[pl.ds(step * seqs + s, 1), :]
        heads_q = jnp.concatenate([own[:, h * head_size : (h + 1) * head_size] for h in range(heads)] * 2, axis=0)
        q8 = heads_q.astype(bf16)
        s_lo = dot(q8, k_ref[s, :half, :], ((1,), (1,)))
        s_hi = dot(q8, k_ref[s, half:, :], ((1,), (1,)))
        scores.append(jnp.where(low_row, s_lo, s_hi) * scale)
    stacked = []
    for s in range(seqs):
        off = off_ref[s]
        off8 = jnp.concatenate([off[:, : positions // 2], off[:, positions // 2 :]], axis=0)
        stacked += [off8[:, b * LANES : (b + 1) * LANES] for b in range(off_blocks)]
    high, low = split2(jnp.concatenate(stacked, axis=0))
    wide = dot(high, spread) + dot(low, spread)
    keep_rows, valids, stops = [], [], []
    for s in range(seqs):
        start = s * off_blocks
        offsets = jnp.concatenate(
            [wide[(start + b) * both : (start + b + 1) * both] for b in range(off_blocks)], axis=1
        )
        logits = scores[s] + offsets
        valid = mine & (place < lengths[step * seqs + s])
        tail = jnp.log(1.0 + jnp.exp(-jnp.abs(logits)))
        stops.append(jnp.minimum(logits, 0.0) - tail)
        keep = jnp.where(valid, -jnp.maximum(logits, 0.0) - tail, 0.0)
        keep_rows += [keep[:, b * LANES : (b + 1) * LANES] for b in range(blocks)]
        valids.append(valid)
    high, low = split2(jnp.concatenate(keep_rows, axis=0))
    sums = dot(high, tri) + dot(low, tri)
    top_row = lax.broadcasted_iota(jnp.int32, (both, LANES), 0) < heads
    for s in range(seqs):
        after = [None] * blocks
        running = jnp.zeros((both, LANES), f32)
        for b in reversed(range(blocks)):
            base = (s * blocks + b) * both
            after[b] = sums[base : base + both, :LANES] + running
            running = running + sums[base : base + both, LANES:]
        upper = jnp.where(top_row, pltpu.roll(running, heads, 0), 0.0)
        after_sum = jnp.concatenate([a + upper for a in after], axis=1)
        sticks = jnp.where(valids[s], jnp.exp(stops[s] + after_sum), 0.0).astype(bf16)
        o_lo = dot(sticks, v_ref[s, :half, :])
        o_hi = dot(sticks, v_ref[s, half:, :])
        out = o_lo + pltpu.roll(o_hi, heads, 0)
        for h in range(heads):
            heads_ref[step, s : s + 1, h * head_size : (h + 1) * head_size] = out[h : h + 1]

    @pl.when(step == pl.num_programs(0) - 1)
    def _():
        values = jnp.concatenate([heads_ref[i] for i in range(heads_ref.shape[0])], axis=0)
        width = values.shape[1]
        out_ref[:, :width] = (values * gain_ref[...].astype(f32)).astype(bf16)
        square = jnp.sum(values * values, axis=1, keepdims=True)
        first, second, third = [p.astype(f32) for p in split3(square)]
        lane = lax.broadcasted_iota(jnp.int32, (values.shape[0], LANES), 1)
        extra = jnp.where(lane == 0, first, jnp.where(lane == 1, second, jnp.where(lane == 2, third, 0.0)))
        out_ref[:, width:] = extra.astype(bf16)


def load_kernel(lengths, cache_hbm, out_ref, sem, *, key_heads, chunk, clear):
    count, rows, head_size = out_ref.shape
    per = chunk * key_heads
    chunks = rows // per

    def window(c):
        return pl.ds(pl.multiple_of(c * per, per), per)

    def copy(s, c):
        return pltpu.make_async_copy(cache_hbm.at[s, window(c)], out_ref.at[s, window(c)], sem)

    def live(s):
        return (lengths[s] + chunk - 1) // chunk

    @pl.loop(0, count)
    def _(s):
        @pl.loop(0, live(s))
        def _(c):
            copy(s, c).start()

    if clear:

        @pl.loop(0, count)
        def _(s):
            @pl.loop(live(s), chunks)
            def _(c):
                out_ref[s, window(c), :] = jnp.zeros((per, head_size), bf16)

    @pl.loop(0, count)
    def _(s):
        @pl.loop(0, live(s))
        def _(c):
            copy(s, c).wait()


def load(cache, lengths, clear, limit):
    seq_count, positions, key_heads, head_size = cache.shape
    rows = positions * key_heads
    shape = (seq_count, rows, head_size)

    def kernel(*refs):
        load_kernel(*refs, key_heads=key_heads, chunk=min(positions, 256), clear=clear)

    return pl.pallas_call(
        kernel,
        out_shape=pltpu.VMEM(shape, bf16),
        in_specs=[pl.BlockSpec(memory_space=pltpu.SMEM), pl.BlockSpec(memory_space=pltpu.HBM)],
        out_specs=pl.BlockSpec(memory_space=pltpu.VMEM),
        scratch_shapes=[pltpu.SemaphoreType.DMA(())],
        compiler_params=pltpu.CompilerParams(vmem_limit_bytes=limit * 1024 * 1024),
        name="load_cache",
    )(lengths, pltpu.with_memory_space_constraint(cache.reshape(shape), pltpu.HBM))


def load_weights(weights):
    def kernel(*refs):
        count = len(weights)
        sources, targets, sems = refs[:count], refs[count : 2 * count], refs[-1]
        copies = [pltpu.make_async_copy(a, b, sems.at[i]) for i, (a, b) in enumerate(zip(sources, targets))]
        for copy in copies:
            copy.start()
        for copy in copies:
            copy.wait()

    return pl.pallas_call(
        kernel,
        out_shape=tuple(pltpu.VMEM(w.shape, w.dtype) for w in weights),
        in_specs=[pl.BlockSpec(memory_space=pltpu.HBM)] * len(weights),
        out_specs=tuple(pl.BlockSpec(memory_space=pltpu.VMEM) for _ in weights),
        scratch_shapes=[pltpu.SemaphoreType.DMA((len(weights),))],
        compiler_params=pltpu.CompilerParams(vmem_limit_bytes=4 * 1024 * 1024),
        name="load_weights",
    )(*[pltpu.with_memory_space_constraint(w, pltpu.HBM) for w in weights])


def merge_kernel(starts, kept_ref, other_ref, shared_ref, keep_ref, send_ref):
    _, cols = keep_ref.shape
    seqs = shared_ref.shape[0]
    for target, i in ((send_ref, 1), (keep_ref, 0)):
        window = pl.ds(pl.multiple_of(starts[i], LANES), cols)
        total = kept_ref[:, window].astype(f32) + other_ref[:, window].astype(f32)
        first = total[:seqs] + shared_ref[:, window]
        target[...] = jnp.concatenate([first, total[seqs:]], axis=0).astype(target.dtype)


def merge(starts, kept, other, shared, cols):
    rows = kept.shape[0]
    return pl.pallas_call(
        merge_kernel,
        out_shape=(jax.ShapeDtypeStruct((rows, cols), f32), jax.ShapeDtypeStruct((rows, cols), bf16)),
        grid_spec=pltpu.PrefetchScalarGridSpec(
            num_scalar_prefetch=1,
            grid=(1,),
            in_specs=[whole(kept.shape), whole(other.shape), whole(shared.shape)],
            out_specs=(whole((rows, cols)), whole((rows, cols))),
        ),
        compiler_params=pltpu.CompilerParams(vmem_limit_bytes=8 * 1024 * 1024),
        name="merge",
    )(starts, kept, other, shared)


def attend(queries, keys, values, offsets, lengths, head_gain):
    seq_count, rows, head_size = keys.shape
    heads, positions = offsets.shape[1:]
    key_heads = rows // positions
    seqs = 4
    width = heads * head_size

    def kernel(*refs):
        attend_kernel(*refs, seqs=seqs, heads=heads, key_heads=key_heads)

    return pl.pallas_call(
        kernel,
        out_shape=jax.ShapeDtypeStruct((seq_count, width + LANES), bf16),
        grid_spec=pltpu.PrefetchScalarGridSpec(
            num_scalar_prefetch=1,
            grid=(seq_count // seqs,),
            in_specs=[
                pl.BlockSpec((seq_count, width), lambda i, n: (0, 0)),
                pl.BlockSpec((seqs, rows, head_size), lambda i, n: (i, 0, 0)),
                pl.BlockSpec((seqs, rows, head_size), lambda i, n: (i, 0, 0)),
                pl.BlockSpec((seqs, heads, positions), lambda i, n: (i, 0, 0)),
                pl.BlockSpec((1, width), lambda i, n: (0, 0)),
            ],
            out_specs=pl.BlockSpec((seq_count, width + LANES), lambda i, n: (0, 0)),
            scratch_shapes=[pltpu.VMEM((seq_count // seqs, seqs, width), f32)],
        ),
        compiler_params=pltpu.CompilerParams(
            dimension_semantics=("arbitrary",), vmem_limit_bytes=20 * 1024 * 1024
        ),
        cost_estimate=pl.CostEstimate(flops=2 * 10**9, transcendentals=10**6, bytes_accessed=2 * 10**7),
        name="stick_attend",
    )(
        lengths,
        queries,
        pltpu.with_memory_space_constraint(keys, pltpu.VMEM),
        pltpu.with_memory_space_constraint(values, pltpu.HBM),
        offsets,
        head_gain.reshape(1, width),
    )


def whole(shape):
    return pl.BlockSpec(shape, lambda *_: tuple(0 for _ in shape))


def project_kernel(rows_ref, *refs):
    weights, out_ref = refs[:-1], refs[-1]
    block = weights[0].shape[0]
    total = None
    for i, weight in enumerate(weights):
        piece = dot(rows_ref[:, i * block : (i + 1) * block], weight[...])
        total = piece if total is None else total + piece
    out_ref[...] = total.astype(bf16)


def project(rows, weights):
    shape = (rows.shape[0], weights[0].shape[1])
    return pl.pallas_call(
        project_kernel,
        out_shape=jax.ShapeDtypeStruct(shape, bf16),
        in_specs=[whole(rows.shape)] + [whole(w.shape) for w in weights],
        out_specs=whole(shape),
        grid=(1,),
        compiler_params=pltpu.CompilerParams(vmem_limit_bytes=8 * 1024 * 1024),
        name="project",
    )(rows, *weights)


def out_kernel(*refs, count, width, extra):
    messages, weights, out_ref = refs[:count], refs[count:-1], refs[-1]
    rows = jnp.concatenate([m[:, :width] for m in messages], axis=0)
    pieces = [dot(rows, weight[...], ((1,), (1,))).astype(bf16) for weight in weights]
    pieces.append(jnp.concatenate([m[:, width : width + extra] for m in messages], axis=0))
    out_ref[...] = jnp.concatenate(pieces, axis=1)


def out_project(messages, weights, width, extra):
    rows = sum(m.shape[0] for m in messages)
    shape = (rows, sum(w.shape[0] for w in weights) + extra)

    def kernel(*refs):
        out_kernel(*refs, count=len(messages), width=width, extra=extra)

    return pl.pallas_call(
        kernel,
        out_shape=jax.ShapeDtypeStruct(shape, bf16),
        in_specs=[whole(m.shape) for m in messages] + [whole(w.shape) for w in weights],
        out_specs=whole(shape),
        grid=(1,),
        compiler_params=pltpu.CompilerParams(vmem_limit_bytes=8 * 1024 * 1024),
        name="out_project",
    )(*messages, *weights)


def experts_kernel(place, rows_ref, gain_ref, router_ref, *refs, model, experts, groups):
    gates, ups, downs, out_ref = refs[:groups], refs[groups : 2 * groups], refs[2 * groups : 3 * groups], refs[-1]
    data = rows_ref[:, :model].astype(f32)
    factor = lax.rsqrt(jnp.sum(data * data, axis=-1, keepdims=True) * (1.0 / model) + epsilon)
    normed = (data * factor * gain_ref[...].astype(f32)).astype(bf16)
    mask = rows_ref[:, model:].astype(f32)[:, :experts]
    prob = jax.nn.sigmoid(dot(normed, router_ref[...], ((1,), (1,)))) * mask
    weight = routed_scale * prob / jnp.sum(prob, axis=-1, keepdims=True)
    lane = lax.broadcasted_iota(jnp.int32, weight.shape, 1)
    total = None
    for g in range(groups):
        for e in range(gates[g].shape[0]):
            expert = place[g] * gates[g].shape[0] + e
            mine = jnp.sum(jnp.where(lane == expert, weight, 0.0), axis=-1, keepdims=True)
            gate = dot(normed, gates[g][e])
            up = dot(normed, ups[g][e])
            hidden = (gate / (1.0 + jnp.exp(-gate)) * up).astype(bf16)
            piece = dot(hidden, downs[g][e]) * mine
            total = piece if total is None else total + piece
    out_ref[...] = total.astype(bf16)


def run_experts(rows, gain, router, gates, ups, downs, place):
    count = rows.shape[0]
    model = gates[0].shape[1]
    shape = (count, model)

    def kernel(*refs):
        experts_kernel(*refs, model=model, experts=router.shape[0], groups=len(gates))

    return pl.pallas_call(
        kernel,
        out_shape=jax.ShapeDtypeStruct(shape, bf16),
        grid_spec=pltpu.PrefetchScalarGridSpec(
            num_scalar_prefetch=1,
            grid=(1,),
            in_specs=[whole(rows.shape), whole((1, model)), whole(router.shape)]
            + [pl.BlockSpec(memory_space=pltpu.VMEM)] * (3 * len(gates)),
            out_specs=whole(shape),
        ),
        compiler_params=pltpu.CompilerParams(vmem_limit_bytes=12 * 1024 * 1024),
        name="routed_experts",
    )(
        place,
        rows,
        gain.reshape(1, model),
        router,
        *[pltpu.with_memory_space_constraint(w, pltpu.VMEM) for w in (*gates, *ups, *downs)],
    )


def make_body(n_ep, n_tp):
    inner = 1 << ((n_ep.bit_length() - 1) // 2)
    outer = n_ep // inner
    masks = [1 << i for i in reversed(range(inner.bit_length() - 1))]

    def swap(value, mask):
        return lax.ppermute(value, "ep", [(i, i ^ mask) for i in range(n_ep)])

    def outer_swap(value, k):
        return swap(value, k * inner)

    def tp_swap(value):
        return lax.ppermute(value, "tp", [(i, (i + 1) % n_tp) for i in range(n_tp)])

    def gather(value, over):
        pieces, order = [value], [0]
        for m in over:
            pieces = pieces + [swap(p, m) for p in pieces]
            order = order + [o ^ m for o in order]
        return pieces, order

    def reverse_bits(value):
        result, width = jnp.uint32(0), inner
        while width > 1:
            result = (result << 1) | (value & 1)
            value = value >> 1
            width = width // 2
        return result

    def cut(value, start, size):
        return lax.dynamic_slice(value, (jnp.uint32(0), start), (value.shape[0], size))

    def body(
        tokens,
        attn_gain,
        query_weight,
        key_weight,
        value_weight,
        out_weight,
        head_gain,
        past_keys,
        past_values,
        break_offset,
        cache_lengths,
        ffn_gain,
        router_weight,
        expert_routes,
        expert_gate,
        expert_up,
        expert_down,
        shared_gate,
        shared_up,
        shared_down,
    ):
        seqs, model = tokens.shape
        experts = router_weight.shape[1]
        block = query_weight.shape[0]
        plane = block * inner
        cols = model // n_tp
        key_cols = key_weight.shape[1]
        heads_width = out_weight.shape[1]
        pad = -experts % LANES

        me = lax.axis_index("ep").astype(jnp.uint32)
        my_tp = lax.axis_index("tp").astype(jnp.uint32)
        my_inner = me & (inner - 1)
        my_outer = me >> (inner.bit_length() - 1)
        marks = [my_outer ^ k for k in range(outer)]
        starts = [m * plane for m in marks]
        blocks_at = [(my_inner ^ o) * block for o in range(inner)]
        back_at = [reverse_bits(my_inner ^ o) * block for o in range(inner)]
        own_start, other_start = my_tp * cols, ((my_tp + 1) & (n_tp - 1)) * cols
        row_starts = [m * (outer * seqs) for m in marks]
        place = jnp.stack([me, me ^ 1]).astype(jnp.int32)
        col_starts = jnp.stack([own_start, other_start]).astype(jnp.int32)
        held = (tokens, starts, row_starts, blocks_at, back_at, own_start, col_starts, place)
        held = lax.optimization_barrier(held)
        tokens, starts, row_starts, blocks_at, back_at, own_start, col_starts, place = held

        query_pieces, order = gather(query_weight, masks)
        got = [cut(tokens, starts[0], plane)] + [outer_swap(cut(tokens, starts[k], plane), k) for k in range(1, outer)]
        group_tokens = jnp.concatenate(got, axis=0)

        def by_order(value):
            return jnp.concatenate([cut(value, blocks_at[o], block) for o in order], axis=1)

        gain_plane = cut(attn_gain.reshape(1, model), starts[0], plane)
        ordered = by_order(group_tokens)
        gained = (ordered.astype(f32) * by_order(gain_plane).astype(f32)).astype(bf16)
        query_part = project(gained, query_pieces)
        late = lax.optimization_barrier(
            (query_part, cache_lengths, out_weight, key_weight, value_weight, expert_gate, expert_up, expert_down)
        )
        query_part, load_lengths, out_weight, key_weight, value_weight, expert_gate, expert_up, expert_down = late
        keys = load(past_keys, load_lengths, False, 4)
        query_got = [query_part[:seqs]] + [
            outer_swap(query_part[k * seqs : (k + 1) * seqs], k) for k in range(1, outer)
        ]
        out_pieces, _ = gather(out_weight, masks)
        rest_pieces, _ = gather(jnp.concatenate([key_weight, value_weight], axis=1), masks)
        gates, ups, downs = [[w, swap(w, 1)] for w in (expert_gate, expert_up, expert_down)]
        wide_tokens = tokens.astype(f32)
        factor = lax.rsqrt(jnp.mean(wide_tokens * wide_tokens, axis=-1, keepdims=True) + epsilon)
        queries = (sum(part.astype(f32) for part in query_got) * factor).astype(bf16).astype(f32)

        lane = lax.broadcasted_iota(jnp.int32, (1, 1, experts + pad), 2)
        routed_mask = jnp.sum((expert_routes[:, :, None] == lane).astype(f32), axis=1).astype(bf16)
        rest_part = project(gained, rest_pieces)

        values = past_values.reshape(keys.shape)
        queries, gates, ups, downs = lax.optimization_barrier((queries, gates, ups, downs))
        scaled = attend(queries, keys, values, break_offset, cache_lengths, head_gain)
        messages = [
            jnp.concatenate([scaled, routed_mask, rest_part[k * seqs : (k + 1) * seqs]], axis=1)
            for k in range(outer)
        ]
        arrived = [messages[0]] + [outer_swap(messages[k], k) for k in range(1, outer)]
        cuts = (heads_width, heads_width + LANES, heads_width + LANES + experts + pad)
        group_mask = jnp.concatenate([m[:, cuts[1] : cuts[2]] for m in arrived], axis=0)
        own_part = out_project(arrived, out_pieces, heads_width, LANES)
        other_part = tp_swap(own_part)
        both = own_part.astype(f32) + other_part.astype(f32)
        square_total = jnp.sum(both[:, plane:], axis=1, keepdims=True)
        attention = both[:, :plane] * lax.rsqrt(square_total / (heads_width * n_tp) + epsilon)
        residual_part = (ordered.astype(f32) + attention).astype(bf16)

        residual_plane = jnp.concatenate([cut(residual_part, back_at[o], block) for o in range(inner)], axis=1)
        residual_plane, gates, ups, downs = lax.optimization_barrier((residual_plane, gates, ups, downs))
        held_weights = load_weights((*gates, *ups, *downs))
        gates, ups, downs = held_weights[:2], held_weights[2:4], held_weights[4:]
        peers = [residual_plane] + [outer_swap(residual_plane, k) for k in range(1, outer)]
        stacked = []
        for k in range(outer):
            stacked += [peers[k][(j ^ k) * seqs : (j ^ k) * seqs + seqs] for j in range(outer)]
        stacked = jnp.concatenate(stacked, axis=0)
        group_rows = jnp.concatenate(
            [lax.dynamic_slice(stacked, (row_starts[p], jnp.uint32(0)), (outer * seqs, plane)) for p in range(outer)]
            + [group_mask],
            axis=1,
        )
        row_pieces, _ = gather(group_rows, masks[:-1])

        arrived, group_rows = lax.optimization_barrier((arrived, group_rows))
        fresh = (sum(m[:, cuts[2] :].astype(f32) for m in arrived) * factor).astype(bf16)

        own_rows = group_rows[:seqs, :model]
        data = own_rows.astype(f32)
        scale = lax.rsqrt(jnp.mean(data * data, axis=-1, keepdims=True) + epsilon)
        own_normed = (data * scale * ffn_gain.astype(f32)).astype(bf16)
        shared_hidden = (
            jax.nn.silu(dot(own_normed, shared_gate)) * dot(own_normed, shared_up)
        ).astype(bf16)
        shared_part = dot(shared_hidden, shared_down)

        router = router_weight.T
        results = [run_experts(piece, ffn_gain, router, gates, ups, downs, place) for piece in row_pieces]

        for m in reversed(masks[1:-1]):
            half = len(results) // 2
            back = [swap(r, m) for r in results[half:]]
            results = [(a.astype(f32) + b.astype(f32)).astype(bf16) for a, b in zip(results[:half], back)]
        kept = results[0]
        other = swap(results[1], masks[0]) if len(results) > 1 else jnp.zeros_like(kept)

        keep, send = merge(col_starts, kept, other, shared_part, cols)
        value = keep + tp_swap(send).astype(f32)
        value_out = value.astype(bf16)
        total = value[:seqs]
        for k in range(1, outer):
            total = total + outer_swap(value_out[k * seqs : (k + 1) * seqs], k).astype(f32)
        mixed = (cut(own_rows, own_start, cols).astype(f32) + total).astype(bf16)
        return mixed, fresh[:, :key_cols], fresh[:, key_cols:]

    return body


def solution(mesh):
    placed = (
        P("ep", None),
        P(),
        P("ep", "tp"),
        P("ep", "tp"),
        P("ep", "tp"),
        P("ep", "tp"),
        P("tp"),
        P("ep", None, "tp", None),
        P("ep", None, "tp", None),
        P("ep", "tp", None),
        P("ep"),
        P(),
        P(),
        P("ep", None),
        P("ep", None, "tp"),
        P("ep", None, "tp"),
        P("ep", "tp", None),
        P(None, "tp"),
        P(None, "tp"),
        P("tp", None),
    )
    return jax.shard_map(
        make_body(mesh.shape["ep"], mesh.shape["tp"]),
        mesh=mesh,
        in_specs=placed,
        out_specs=(P("ep", "tp"), P("ep", "tp"), P("ep", "tp")),
        check_vma=False,
    )
```

```python
import jax
import jax.numpy as jnp
from jax import lax
from jax.experimental import pallas as pl
from jax.experimental.pallas import tpu as pltpu
from jax.sharding import PartitionSpec as P


epsilon = 1e-06
routed_scale = 2.5
LANES = 128
bf16 = jnp.bfloat16
f32 = jnp.float32


def dot(a, b, dims=((1,), (0,)), precision=None):
    return lax.dot_general(a, b, (dims, ((), ())), precision=precision, preferred_element_type=f32)


def split3(value):
    high = value.astype(bf16)
    rest = value - high.astype(f32)
    mid = rest.astype(bf16)
    low = (rest - mid.astype(f32)).astype(bf16)
    return high, mid, low


def split2(value):
    high = value.astype(bf16)
    return high, (value - high.astype(f32)).astype(bf16)


def attend_kernel(
    lengths, q_ref, k_hbm, v_hbm, off_ref, gain_ref, mask_ref, out_ref, k_ref, v_ref, heads_ref, sems,
    *, seqs, heads, key_heads
):
    count, rows, head_size = k_ref.shape
    half = rows // 2
    positions = rows // key_heads
    block = LANES * key_heads
    group = heads // key_heads
    both = 2 * heads
    blocks = half // LANES
    off_blocks = positions // 2 // LANES

    def key_copy(s):
        live = pl.multiple_of((lengths[s] * key_heads + LANES - 1) // LANES * LANES, LANES)
        window = pl.ds(0, live)
        return pltpu.make_async_copy(k_hbm.at[s, window], k_ref.at[s, window], sems.at[0, s])

    def value_copy(s):
        return pltpu.make_async_copy(v_hbm.at[s], v_ref.at[s], sems.at[1, s])

    for first in range(0, count, seqs):
        for s in range(first, first + seqs):
            key_copy(s).start()
        for s in range(first, first + seqs):
            value_copy(s).start()

    row = lax.broadcasted_iota(jnp.int32, (both, half), 0)
    col = lax.broadcasted_iota(jnp.int32, (both, half), 1)
    place = jnp.where(row >= heads, positions // 2, 0) + col // key_heads
    mine = (col % key_heads) == ((row % heads) // group)
    place = jnp.where(mine, place, positions)
    low_row = row < heads
    scale = head_size ** (-0.5)
    spread = (
        lax.broadcasted_iota(jnp.int32, (LANES, block), 1) // key_heads
        == lax.broadcasted_iota(jnp.int32, (LANES, block), 0)
    ).astype(bf16)
    tri_row = lax.broadcasted_iota(jnp.int32, (LANES, 2 * LANES), 0)
    tri_col = lax.broadcasted_iota(jnp.int32, (LANES, 2 * LANES), 1)
    tri = ((tri_row > tri_col) | (tri_col >= LANES)).astype(bf16)
    top_row = lax.broadcasted_iota(jnp.int32, (both, LANES), 0) < heads

    for first in range(0, count, seqs):
        members = range(first, first + seqs)
        for s in members:
            key_copy(s).wait()
        scores = []
        for s in members:
            own = q_ref[s : s + 1, :]
            q8 = jnp.concatenate(
                [own[:, h * head_size : (h + 1) * head_size] for h in range(heads)] * 2, axis=0
            ).astype(bf16)
            s_lo = dot(q8, k_ref[s, :half, :], ((1,), (1,)))
            s_hi = dot(q8, k_ref[s, half:, :], ((1,), (1,)))
            scores.append(jnp.where(low_row, s_lo, s_hi) * scale)
        stacked = []
        for s in members:
            off = off_ref[s]
            off8 = jnp.concatenate([off[:, : positions // 2], off[:, positions // 2 :]], axis=0)
            stacked += [off8[:, b * LANES : (b + 1) * LANES] for b in range(off_blocks)]
        high, low = split2(jnp.concatenate(stacked, axis=0))
        wide = dot(high, spread) + dot(low, spread)
        keep_rows, valids, stops = [], [], []
        for i, s in enumerate(members):
            start = i * off_blocks
            offsets = jnp.concatenate(
                [wide[(start + b) * both : (start + b + 1) * both] for b in range(off_blocks)], axis=1
            )
            logits = scores[i] + offsets
            valid = place < lengths[s]
            tail = jnp.log(1.0 + jnp.exp(-jnp.abs(logits)))
            stops.append(jnp.minimum(logits, 0.0) - tail)
            keep = jnp.where(valid, -jnp.maximum(logits, 0.0) - tail, 0.0)
            keep_rows += [keep[:, b * LANES : (b + 1) * LANES] for b in range(blocks)]
            valids.append(valid)
        high, low = split2(jnp.concatenate(keep_rows, axis=0))
        sums = dot(high, tri) + dot(low, tri)
        sticks = []
        for i in range(seqs):
            after = [None] * blocks
            running = jnp.zeros((both, LANES), f32)
            for b in reversed(range(blocks)):
                base = (i * blocks + b) * both
                after[b] = sums[base : base + both, :LANES] + running
                running = running + sums[base : base + both, LANES:]
            upper = jnp.where(top_row, pltpu.roll(running, heads, 0), 0.0)
            after_sum = jnp.concatenate([a + upper for a in after], axis=1)
            sticks.append(jnp.where(valids[i], jnp.exp(stops[i] + after_sum), 0.0).astype(bf16))
        for s in members:
            value_copy(s).wait()
        for i, s in enumerate(members):
            o_lo = dot(sticks[i], v_ref[s, :half, :])
            o_hi = dot(sticks[i], v_ref[s, half:, :])
            out = o_lo + pltpu.roll(o_hi, heads, 0)
            for h in range(heads):
                heads_ref[s : s + 1, h * head_size : (h + 1) * head_size] = out[h : h + 1]

    values = heads_ref[...]
    width = values.shape[1]
    out_ref[:, :width] = (values * gain_ref[...].astype(f32)).astype(bf16)
    square = jnp.sum(values * values, axis=1, keepdims=True)
    first, second, third = [p.astype(f32) for p in split3(square)]
    lane = lax.broadcasted_iota(jnp.int32, (values.shape[0], LANES), 1)
    extra = jnp.where(lane == 0, first, jnp.where(lane == 1, second, jnp.where(lane == 2, third, 0.0)))
    out_ref[:, width : width + LANES] = extra.astype(bf16)
    out_ref[:, width + LANES :] = mask_ref[...]


def load_weights(weights):
    def kernel(*refs):
        count = len(weights)
        sources, targets, sems = refs[:count], refs[count : 2 * count], refs[-1]
        copies = [pltpu.make_async_copy(a, b, sems.at[i]) for i, (a, b) in enumerate(zip(sources, targets))]
        for copy in copies:
            copy.start()
        for copy in copies:
            copy.wait()

    return pl.pallas_call(
        kernel,
        out_shape=tuple(pltpu.VMEM(w.shape, w.dtype) for w in weights),
        in_specs=[pl.BlockSpec(memory_space=pltpu.HBM)] * len(weights),
        out_specs=tuple(pl.BlockSpec(memory_space=pltpu.VMEM) for _ in weights),
        scratch_shapes=[pltpu.SemaphoreType.DMA((len(weights),))],
        compiler_params=pltpu.CompilerParams(vmem_limit_bytes=4 * 1024 * 1024),
        name="load_weights",
    )(*[pltpu.with_memory_space_constraint(w, pltpu.HBM) for w in weights])


def attend(queries, key_cache, value_cache, offsets, lengths, gain_row, mask):
    seq_count, positions, key_heads, head_size = key_cache.shape
    heads = offsets.shape[1]
    rows = positions * key_heads
    shape = (seq_count, rows, head_size)
    width = heads * head_size
    total = width + LANES + mask.shape[1]
    hbm = pl.BlockSpec(memory_space=pltpu.HBM)

    def kernel(*refs):
        attend_kernel(*refs, seqs=8, heads=heads, key_heads=key_heads)

    return pl.pallas_call(
        kernel,
        out_shape=jax.ShapeDtypeStruct((seq_count, total), bf16),
        grid_spec=pltpu.PrefetchScalarGridSpec(
            num_scalar_prefetch=1,
            grid=(1,),
            in_specs=[whole((seq_count, width)), hbm, hbm, whole(offsets.shape), whole((1, width)), whole(mask.shape)],
            out_specs=whole((seq_count, total)),
            scratch_shapes=[
                pltpu.VMEM(shape, bf16),
                pltpu.VMEM(shape, bf16),
                pltpu.VMEM((seq_count, width), f32),
                pltpu.SemaphoreType.DMA((2, seq_count)),
            ],
        ),
        compiler_params=pltpu.CompilerParams(vmem_limit_bytes=24 * 1024 * 1024),
        cost_estimate=pl.CostEstimate(flops=2 * 10**9, transcendentals=10**6, bytes_accessed=2 * 10**7),
        name="stick_attend",
    )(
        lengths,
        queries,
        pltpu.with_memory_space_constraint(key_cache.reshape(shape), pltpu.HBM),
        pltpu.with_memory_space_constraint(value_cache.reshape(shape), pltpu.HBM),
        pltpu.with_memory_space_constraint(offsets, pltpu.VMEM),
        gain_row,
        mask,
    )


def pack(arrays, other):
    widths = [a.shape[1] for a in arrays]
    shape = (arrays[0].shape[0], sum(widths))

    def kernel(*refs):
        out_ref, second_ref, sems = refs[-3:]
        copies = [pltpu.make_async_copy(refs[-4], second_ref, sems.at[len(arrays)])]
        for i, ref in enumerate(refs[:-4]):
            window = pl.ds(sum(widths[:i]), widths[i])
            copies.append(pltpu.make_async_copy(ref, out_ref.at[:, window], sems.at[i]))
        for copy in copies:
            copy.start()
        for copy in copies:
            copy.wait()

    return pl.pallas_call(
        kernel,
        out_shape=(pltpu.VMEM(shape, bf16), pltpu.VMEM(other.shape, other.dtype)),
        in_specs=[pl.BlockSpec(memory_space=pltpu.HBM)] * (len(arrays) + 1),
        out_specs=(pl.BlockSpec(memory_space=pltpu.VMEM), pl.BlockSpec(memory_space=pltpu.VMEM)),
        scratch_shapes=[pltpu.SemaphoreType.DMA((len(arrays) + 1,))],
        compiler_params=pltpu.CompilerParams(vmem_limit_bytes=4 * 1024 * 1024),
        name="pack",
    )(*[pltpu.with_memory_space_constraint(a, pltpu.HBM) for a in (*arrays, other)])


def whole(shape):
    return pl.BlockSpec(shape, lambda *_: tuple(0 for _ in shape))


def project(rows, weights, skip=0):
    block, width = weights[0].shape
    shape = (rows.shape[0], width - skip)

    def kernel(rows_ref, *refs):
        total = None
        for i, weight in enumerate(refs[:-1]):
            piece = dot(rows_ref[:, i * block : (i + 1) * block], weight[:, skip:])
            total = piece if total is None else total + piece
        refs[-1][...] = total.astype(bf16)

    return pl.pallas_call(
        kernel,
        out_shape=jax.ShapeDtypeStruct(shape, bf16),
        in_specs=[whole(rows.shape)] + [whole(w.shape) for w in weights],
        out_specs=whole(shape),
        grid=(1,),
        compiler_params=pltpu.CompilerParams(vmem_limit_bytes=8 * 1024 * 1024),
        name="project",
    )(rows, *weights)


def out_kernel(*refs, count, width, extra):
    messages, weights, out_ref = refs[:count], refs[count:-1], refs[-1]
    rows = jnp.concatenate([m[:, :width] for m in messages], axis=0)
    pieces = [dot(rows, weight[:, :width], ((1,), (1,))).astype(bf16) for weight in weights]
    pieces.append(jnp.concatenate([m[:, width : width + extra] for m in messages], axis=0))
    out_ref[...] = jnp.concatenate(pieces, axis=1)


def out_project(messages, weights, width, extra):
    rows = sum(m.shape[0] for m in messages)
    shape = (rows, sum(w.shape[0] for w in weights) + extra)

    def kernel(*refs):
        out_kernel(*refs, count=len(messages), width=width, extra=extra)

    return pl.pallas_call(
        kernel,
        out_shape=jax.ShapeDtypeStruct(shape, bf16),
        in_specs=[whole(m.shape) for m in messages] + [whole(w.shape) for w in weights],
        out_specs=whole(shape),
        grid=(1,),
        compiler_params=pltpu.CompilerParams(vmem_limit_bytes=8 * 1024 * 1024),
        name="out_project",
    )(*messages, *weights)


def experts_kernel(place, rows_ref, gain_ref, router_ref, *refs, model, experts, groups, cols, seqs):
    gates, ups, downs = refs[:groups], refs[groups : 2 * groups], refs[2 * groups : 3 * groups]
    shared = refs[3 * groups : -3]
    keep_ref, send_ref, total_ref = refs[-3:]
    data = rows_ref[:, :model].astype(f32)
    factor = lax.rsqrt(jnp.sum(data * data, axis=-1, keepdims=True) * (1.0 / model) + epsilon)
    normed = (data * factor * gain_ref[...].astype(f32)).astype(bf16)
    mask = rows_ref[:, model:].astype(f32)[:, :experts]
    prob = jax.nn.sigmoid(dot(normed, router_ref[...], ((1,), (1,)))) * mask
    weight = routed_scale * prob / jnp.sum(prob, axis=-1, keepdims=True)
    lane = lax.broadcasted_iota(jnp.int32, weight.shape, 1)
    total = None
    for g in range(groups):
        for e in range(gates[g].shape[0]):
            expert = place[g] * gates[g].shape[0] + e
            mine = jnp.sum(jnp.where(lane == expert, weight, 0.0), axis=-1, keepdims=True)
            gate = dot(normed, gates[g][e])
            up = dot(normed, ups[g][e])
            hidden = (gate / (1.0 + jnp.exp(-gate)) * up).astype(bf16)
            piece = dot(hidden, downs[g][e]) * mine
            total = piece if total is None else total + piece
    total_ref[...] = total
    if shared:
        gate = dot(normed[:seqs], shared[0][...])
        up = dot(normed[:seqs], shared[1][...])
        hidden = (gate / (1.0 + jnp.exp(-gate)) * up).astype(bf16)
        total_ref[:seqs] = total[:seqs] + dot(hidden, shared[2][...])
    for target, i in ((send_ref, 1), (keep_ref, 0)):
        window = pl.ds(pl.multiple_of(place[groups + i], LANES), cols)
        target[...] = total_ref[:, window].astype(target.dtype)


def run_experts(rows, gain, router, gates, ups, downs, place, cols, seqs, shared=()):
    count = rows.shape[0]
    model = gates[0].shape[1]

    def kernel(*refs):
        experts_kernel(*refs, model=model, experts=router.shape[0], groups=len(gates), cols=cols, seqs=seqs)

    return pl.pallas_call(
        kernel,
        out_shape=(jax.ShapeDtypeStruct((count, cols), f32), jax.ShapeDtypeStruct((count, cols), bf16)),
        grid_spec=pltpu.PrefetchScalarGridSpec(
            num_scalar_prefetch=1,
            grid=(1,),
            in_specs=[whole(rows.shape), whole((1, model)), whole(router.shape)]
            + [pl.BlockSpec(memory_space=pltpu.VMEM)] * (3 * len(gates) + len(shared)),
            out_specs=(whole((count, cols)), whole((count, cols))),
            scratch_shapes=[pltpu.VMEM((count, model), f32)],
        ),
        compiler_params=pltpu.CompilerParams(vmem_limit_bytes=12 * 1024 * 1024),
        name="routed_experts",
    )(
        place,
        rows,
        gain,
        router,
        *[pltpu.with_memory_space_constraint(w, pltpu.VMEM) for w in (*gates, *ups, *downs, *shared)],
    )


def make_body(n_ep, n_tp):
    inner = 1 << ((n_ep.bit_length() - 1) // 2)
    outer = n_ep // inner
    masks = [1 << i for i in reversed(range(inner.bit_length() - 1))]

    def swap(value, mask):
        return lax.ppermute(value, "ep", [(i, i ^ mask) for i in range(n_ep)])

    def outer_swap(value, k):
        return swap(value, k * inner)

    def outer_exchange(messages):
        got = {}
        for k in reversed(range(1, outer)):
            got[k] = outer_swap(messages[k], k)
        return [messages[0]] + [got[k] for k in range(1, outer)]

    def tp_swap(value):
        return lax.ppermute(value, "tp", [(i, (i + 1) % n_tp) for i in range(n_tp)])

    def gather(value, over):
        pieces, order = [value], [0]
        for m in over:
            more = []
            for piece in pieces:
                more.append(swap(piece, m))
            pieces = pieces + more
            order = order + [o ^ m for o in order]
        return pieces, order

    def reverse_bits(value):
        result, width = jnp.uint32(0), inner
        while width > 1:
            result = (result << 1) | (value & 1)
            value = value >> 1
            width = width // 2
        return result

    def cut(value, start, size):
        return lax.dynamic_slice(value, (jnp.uint32(0), start), (value.shape[0], size))

    def body(
        tokens,
        attn_gain,
        query_weight,
        key_weight,
        value_weight,
        out_weight,
        head_gain,
        past_keys,
        past_values,
        break_offset,
        cache_lengths,
        ffn_gain,
        router_weight,
        expert_routes,
        expert_gate,
        expert_up,
        expert_down,
        shared_gate,
        shared_up,
        shared_down,
    ):
        seqs, model = tokens.shape
        experts = router_weight.shape[1]
        block = query_weight.shape[0]
        plane = block * inner
        cols = model // n_tp
        key_cols = key_weight.shape[1]
        heads_width = out_weight.shape[1]
        pad = -experts % LANES

        me = lax.axis_index("ep").astype(jnp.uint32)
        my_tp = lax.axis_index("tp").astype(jnp.uint32)
        my_inner = me & (inner - 1)
        my_outer = me >> (inner.bit_length() - 1)
        marks = [my_outer ^ k for k in range(outer)]
        starts = [m * plane for m in marks]
        blocks_at = [(my_inner ^ o) * block for o in range(inner)]
        back_at = [reverse_bits(my_inner ^ o) * block for o in range(inner)]
        own_start, other_start = my_tp * cols, ((my_tp + 1) & (n_tp - 1)) * cols
        row_starts = [m * (outer * seqs) for m in marks]
        place = jnp.stack([me, me ^ 1, own_start, other_start]).astype(jnp.int32)
        held = (tokens, starts, row_starts, blocks_at, back_at, own_start, place)
        held = lax.optimization_barrier(held)
        tokens, starts, row_starts, blocks_at, back_at, own_start, place = held

        query_pieces, order = gather(query_weight, masks)
        got = outer_exchange([cut(tokens, start, plane) for start in starts])
        group_tokens = jnp.concatenate(got, axis=0)

        def by_order(value):
            return jnp.concatenate([cut(value, blocks_at[o], block) for o in order], axis=1)

        gain_plane = cut(attn_gain.reshape(1, model), starts[0], plane)
        ordered = by_order(group_tokens)
        gained = (ordered.astype(f32) * by_order(gain_plane).astype(f32)).astype(bf16)
        query_pieces[0] = load_weights([query_weight])[0]
        query_part = project(gained, query_pieces)
        lane = lax.broadcasted_iota(jnp.int32, (1, 1, experts + pad), 2)
        query_part, routes, gains, late_tokens, packs = lax.optimization_barrier(
            (query_part, expert_routes, (head_gain, ffn_gain), tokens, (out_weight, key_weight, value_weight))
        )
        query_got = outer_exchange([query_part[k * seqs : (k + 1) * seqs] for k in range(outer)])
        routed_mask = jnp.sum((routes[:, :, None] == lane).astype(f32), axis=1).astype(bf16)
        gain_row = gains[0].reshape(1, -1)
        ffn_row = gains[1].reshape(1, -1)
        wide_tokens = late_tokens.astype(f32)
        factor = lax.rsqrt(jnp.mean(wide_tokens * wide_tokens, axis=-1, keepdims=True) + epsilon)
        packed, offsets = pack(packs, break_offset)
        late_pieces, _ = gather(packed, masks[:-1])
        queries = (sum(part.astype(f32) for part in query_got) * factor).astype(bf16).astype(f32)

        held = lax.optimization_barrier((queries, expert_gate, expert_up, expert_down))
        queries, expert_gate, expert_up, expert_down = held
        gates, ups, downs = [[w, swap(w, 1)] for w in (expert_gate, expert_up, expert_down)]
        scaled = attend(
            queries, past_keys, past_values, offsets, cache_lengths, gain_row, routed_mask
        )
        held = lax.optimization_barrier((scaled, gates, ups, downs, late_pieces))
        scaled, gates, ups, downs, late_pieces = held
        late_pieces = late_pieces + [swap(p, masks[-1]) for p in late_pieces]
        arrived = outer_exchange([scaled] * outer)
        group_mask = jnp.concatenate([m[:, heads_width + LANES :] for m in arrived], axis=0)
        own_part = out_project(arrived, late_pieces, heads_width, LANES)
        own_part, *shared = lax.optimization_barrier((own_part, shared_gate, shared_up, shared_down))
        shared = load_weights(shared)
        other_part = tp_swap(own_part)
        both = own_part.astype(f32) + other_part.astype(f32)
        square_total = jnp.sum(both[:, plane:], axis=1, keepdims=True)
        attention = both[:, :plane] * lax.rsqrt(square_total / (heads_width * n_tp) + epsilon)
        residual_part = (ordered.astype(f32) + attention).astype(bf16)

        residual_plane = jnp.concatenate([cut(residual_part, back_at[o], block) for o in range(inner)], axis=1)
        held = lax.optimization_barrier((residual_plane, gates, ups, downs, gained, shared))
        residual_plane, gates, ups, downs, gained, shared = held
        held_weights = load_weights((*gates, *ups, *downs))
        gates, ups, downs = held_weights[:2], held_weights[2:4], held_weights[4:]
        peers = outer_exchange([residual_plane] * outer)
        stacked = []
        for k in range(outer):
            stacked += [peers[k][(j ^ k) * seqs : (j ^ k) * seqs + seqs] for j in range(outer)]
        stacked = jnp.concatenate(stacked, axis=0)
        group_rows = jnp.concatenate(
            [lax.dynamic_slice(stacked, (row_starts[p], jnp.uint32(0)), (outer * seqs, plane)) for p in range(outer)]
            + [group_mask],
            axis=1,
        )
        group_rows, gates, ups, downs = lax.optimization_barrier((group_rows, gates, ups, downs))
        row_pieces, _ = gather(group_rows, masks[:-1])

        rest_part = project(gained, late_pieces, heads_width)
        rest_got = outer_exchange([rest_part[k * seqs : (k + 1) * seqs] for k in range(outer)])
        fresh = (sum(part.astype(f32) for part in rest_got) * factor).astype(bf16)
        own_rows = group_rows[:seqs, :model]

        router = router_weight.T
        results = []
        for i, piece in enumerate(row_pieces):
            if i > 0:
                piece, results = lax.optimization_barrier((piece, results))
            extra = shared if i == 0 else ()
            results.append(run_experts(piece, ffn_row, router, gates, ups, downs, place, cols, seqs, extra))
        sums = []
        for pair in results:
            sums.append(pair[0] + tp_swap(pair[1]).astype(f32))
        for m in reversed(masks[:-1]):
            half = len(sums) // 2
            back = [swap(v.astype(bf16), m) for v in sums[half:]]
            sums = [a + b.astype(f32) for a, b in zip(sums[:half], back)]
        value = sums[0]
        value_out = value.astype(bf16)
        parts = outer_exchange([value_out[k * seqs : (k + 1) * seqs] for k in range(outer)])
        total = value[:seqs] + sum(part.astype(f32) for part in parts[1:])
        mixed = (cut(own_rows, own_start, cols).astype(f32) + total).astype(bf16)
        return mixed, fresh[:, :key_cols], fresh[:, key_cols:]

    return body


def solution(mesh):
    placed = (
        P("ep", None),
        P(),
        P("ep", "tp"),
        P("ep", "tp"),
        P("ep", "tp"),
        P("ep", "tp"),
        P("tp"),
        P("ep", None, "tp", None),
        P("ep", None, "tp", None),
        P("ep", "tp", None),
        P("ep"),
        P(),
        P(),
        P("ep", None),
        P("ep", None, "tp"),
        P("ep", None, "tp"),
        P("ep", "tp", None),
        P(None, "tp"),
        P(None, "tp"),
        P("tp", None),
    )
    n_ep = mesh.shape["ep"]
    step = make_body(n_ep, mesh.shape["tp"])

    return jax.shard_map(
        step,
        mesh=mesh,
        in_specs=placed,
        out_specs=(P("ep", "tp"), P("ep", "tp"), P("ep", "tp")),
        check_vma=False,
    )
```

```python
import jax
import jax.numpy as jnp
from jax import lax
from jax.experimental import pallas as pl
from jax.experimental.pallas import tpu as pltpu
from jax.sharding import PartitionSpec as P


epsilon = 1e-06
routed_scale = 2.5
LANES = 128
bf16 = jnp.bfloat16
f32 = jnp.float32


def dot(a, b, dims=((1,), (0,)), precision=None):
    return lax.dot_general(a, b, (dims, ((), ())), precision=precision, preferred_element_type=f32)


def split3(value):
    high = value.astype(bf16)
    rest = value - high.astype(f32)
    mid = rest.astype(bf16)
    low = (rest - mid.astype(f32)).astype(bf16)
    return high, mid, low


def split2(value):
    high = value.astype(bf16)
    return high, (value - high.astype(f32)).astype(bf16)


def attend_kernel(
    lengths, q_ref, k_hbm, v_hbm, off_ref, gain_ref, mask_ref, out_ref, k_ref, v_ref, heads_ref, sems,
    *, seqs, heads, key_heads
):
    count, rows, head_size = k_ref.shape
    half = rows // 2
    positions = rows // key_heads
    block = LANES * key_heads
    group = heads // key_heads
    both = 2 * heads
    blocks = half // LANES
    off_blocks = positions // 2 // LANES

    def key_copy(s):
        live = pl.multiple_of((lengths[s] * key_heads + LANES - 1) // LANES * LANES, LANES)
        window = pl.ds(0, live)
        return pltpu.make_async_copy(k_hbm.at[s, window], k_ref.at[s, window], sems.at[0, s])

    def value_copy(s):
        return pltpu.make_async_copy(v_hbm.at[s], v_ref.at[s], sems.at[1, s])

    for first in range(0, count, seqs):
        for s in range(first, first + seqs):
            key_copy(s).start()
        for s in range(first, first + seqs):
            value_copy(s).start()

    row = lax.broadcasted_iota(jnp.int32, (both, half), 0)
    col = lax.broadcasted_iota(jnp.int32, (both, half), 1)
    place = jnp.where(row >= heads, positions // 2, 0) + col // key_heads
    mine = (col % key_heads) == ((row % heads) // group)
    place = jnp.where(mine, place, positions)
    low_row = row < heads
    scale = head_size ** (-0.5)
    spread = (
        lax.broadcasted_iota(jnp.int32, (LANES, block), 1) // key_heads
        == lax.broadcasted_iota(jnp.int32, (LANES, block), 0)
    ).astype(bf16)
    tri_row = lax.broadcasted_iota(jnp.int32, (LANES, 2 * LANES), 0)
    tri_col = lax.broadcasted_iota(jnp.int32, (LANES, 2 * LANES), 1)
    tri = ((tri_row > tri_col) | (tri_col >= LANES)).astype(bf16)
    top_row = lax.broadcasted_iota(jnp.int32, (both, LANES), 0) < heads

    for first in range(0, count, seqs):
        members = range(first, first + seqs)
        for s in members:
            key_copy(s).wait()
        scores = []
        for s in members:
            own = q_ref[s : s + 1, :]
            q8 = jnp.concatenate(
                [own[:, h * head_size : (h + 1) * head_size] for h in range(heads)] * 2, axis=0
            ).astype(bf16)
            s_lo = dot(q8, k_ref[s, :half, :], ((1,), (1,)))
            s_hi = dot(q8, k_ref[s, half:, :], ((1,), (1,)))
            scores.append(jnp.where(low_row, s_lo, s_hi) * scale)
        stacked = []
        for s in members:
            off = off_ref[s]
            off8 = jnp.concatenate([off[:, : positions // 2], off[:, positions // 2 :]], axis=0)
            stacked += [off8[:, b * LANES : (b + 1) * LANES] for b in range(off_blocks)]
        high, low = split2(jnp.concatenate(stacked, axis=0))
        wide = dot(high, spread) + dot(low, spread)
        keep_rows, valids, stops = [], [], []
        for i, s in enumerate(members):
            start = i * off_blocks
            offsets = jnp.concatenate(
                [wide[(start + b) * both : (start + b + 1) * both] for b in range(off_blocks)], axis=1
            )
            logits = scores[i] + offsets
            valid = place < lengths[s]
            tail = jnp.log(1.0 + jnp.exp(-jnp.abs(logits)))
            stops.append(jnp.minimum(logits, 0.0) - tail)
            keep = jnp.where(valid, -jnp.maximum(logits, 0.0) - tail, 0.0)
            keep_rows += [keep[:, b * LANES : (b + 1) * LANES] for b in range(blocks)]
            valids.append(valid)
        high, low = split2(jnp.concatenate(keep_rows, axis=0))
        sums = dot(high, tri) + dot(low, tri)
        sticks = []
        for i in range(seqs):
            after = [None] * blocks
            running = jnp.zeros((both, LANES), f32)
            for b in reversed(range(blocks)):
                base = (i * blocks + b) * both
                after[b] = sums[base : base + both, :LANES] + running
                running = running + sums[base : base + both, LANES:]
            upper = jnp.where(top_row, pltpu.roll(running, heads, 0), 0.0)
            after_sum = jnp.concatenate([a + upper for a in after], axis=1)
            sticks.append(jnp.where(valids[i], jnp.exp(stops[i] + after_sum), 0.0).astype(bf16))
        for s in members:
            value_copy(s).wait()
        for i, s in enumerate(members):
            o_lo = dot(sticks[i], v_ref[s, :half, :])
            o_hi = dot(sticks[i], v_ref[s, half:, :])
            out = o_lo + pltpu.roll(o_hi, heads, 0)
            for h in range(heads):
                heads_ref[s : s + 1, h * head_size : (h + 1) * head_size] = out[h : h + 1]

    values = heads_ref[...]
    width = values.shape[1]
    out_ref[:, :width] = (values * gain_ref[...].astype(f32).reshape(1, width)).astype(bf16)
    square = jnp.sum(values * values, axis=1, keepdims=True)
    first, second, third = [p.astype(f32) for p in split3(square)]
    lane = lax.broadcasted_iota(jnp.int32, (values.shape[0], LANES), 1)
    extra = jnp.where(lane == 0, first, jnp.where(lane == 1, second, jnp.where(lane == 2, third, 0.0)))
    out_ref[:, width : width + LANES] = extra.astype(bf16)
    out_ref[:, width + LANES :] = mask_ref[...]


def load_weights(weights):
    def kernel(*refs):
        count = len(weights)
        sources, targets, sems = refs[:count], refs[count : 2 * count], refs[-1]
        copies = [pltpu.make_async_copy(a, b, sems.at[i]) for i, (a, b) in enumerate(zip(sources, targets))]
        for copy in copies:
            copy.start()
        for copy in copies:
            copy.wait()

    return pl.pallas_call(
        kernel,
        out_shape=tuple(pltpu.VMEM(w.shape, w.dtype) for w in weights),
        in_specs=[pl.BlockSpec(memory_space=pltpu.HBM)] * len(weights),
        out_specs=tuple(pl.BlockSpec(memory_space=pltpu.VMEM) for _ in weights),
        scratch_shapes=[pltpu.SemaphoreType.DMA((len(weights),))],
        compiler_params=pltpu.CompilerParams(vmem_limit_bytes=4 * 1024 * 1024),
        name="load_weights",
    )(*[pltpu.with_memory_space_constraint(w, pltpu.HBM) for w in weights])


def attend(queries, key_cache, value_cache, offsets, lengths, gain_row, mask):
    seq_count, positions, key_heads, head_size = key_cache.shape
    heads = offsets.shape[1]
    rows = positions * key_heads
    shape = (seq_count, rows, head_size)
    width = heads * head_size
    total = width + LANES + mask.shape[1]
    hbm = pl.BlockSpec(memory_space=pltpu.HBM)

    def kernel(*refs):
        attend_kernel(*refs, seqs=8, heads=heads, key_heads=key_heads)

    return pl.pallas_call(
        kernel,
        out_shape=jax.ShapeDtypeStruct((seq_count, total), bf16),
        grid_spec=pltpu.PrefetchScalarGridSpec(
            num_scalar_prefetch=1,
            grid=(1,),
            in_specs=[whole((seq_count, width)), hbm, hbm, whole(offsets.shape), whole((width,)), whole(mask.shape)],
            out_specs=whole((seq_count, total)),
            scratch_shapes=[
                pltpu.VMEM(shape, bf16),
                pltpu.VMEM(shape, bf16),
                pltpu.VMEM((seq_count, width), f32),
                pltpu.SemaphoreType.DMA((2, seq_count)),
            ],
        ),
        compiler_params=pltpu.CompilerParams(vmem_limit_bytes=24 * 1024 * 1024),
        cost_estimate=pl.CostEstimate(flops=2 * 10**9, transcendentals=10**6, bytes_accessed=2 * 10**7),
        name="stick_attend",
    )(
        pltpu.with_memory_space_constraint(lengths, pltpu.VMEM),
        queries,
        pltpu.with_memory_space_constraint(key_cache.reshape(shape), pltpu.HBM),
        pltpu.with_memory_space_constraint(value_cache.reshape(shape), pltpu.HBM),
        pltpu.with_memory_space_constraint(offsets, pltpu.VMEM),
        pltpu.with_memory_space_constraint(gain_row, pltpu.VMEM),
        mask,
    )


def pack(arrays, others, tokens, routes, lanes):
    widths = [a.shape[1] for a in arrays]
    shape = (arrays[0].shape[0], sum(widths))
    count = len(arrays)
    seqs, model = tokens.shape
    tops = routes.shape[0]

    extra = len(others)

    def kernel(tokens_hbm, routes_hbm, *refs):
        other_refs, refs = refs[:extra], refs[extra:]
        out_ref, factor_ref, mask_ref = refs[count : count + 3]
        targets = refs[count + 3 : count + 3 + extra]
        tokens_ref, routes_ref, sems = refs[count + 3 + extra :]
        early = [
            pltpu.make_async_copy(tokens_hbm, tokens_ref, sems.at[count + extra]),
            pltpu.make_async_copy(routes_hbm, routes_ref, sems.at[count + extra + 1]),
        ]
        for copy in early:
            copy.start()
        copies = [
            pltpu.make_async_copy(source, target, sems.at[count + i])
            for i, (source, target) in enumerate(zip(other_refs, targets))
        ]
        for i, ref in enumerate(refs[:count]):
            window = pl.ds(sum(widths[:i]), widths[i])
            copies.append(pltpu.make_async_copy(ref, out_ref.at[:, window], sems.at[i]))
        for copy in copies:
            copy.start()
        for copy in early:
            copy.wait()
        data = tokens_ref[...].astype(f32)
        factor = lax.rsqrt(jnp.sum(data * data, axis=-1, keepdims=True) * (1.0 / model) + epsilon)
        factor_ref[...] = jnp.broadcast_to(factor, factor_ref.shape)
        slot = lax.broadcasted_iota(jnp.int32, (lanes, seqs), 0)
        chosen = jnp.zeros((lanes, seqs), f32)
        for i in range(tops):
            chosen = chosen + jnp.where(routes_ref[i : i + 1, :] == slot, 1.0, 0.0)
        eye = (
            lax.broadcasted_iota(jnp.int32, (lanes, lanes), 0) == lax.broadcasted_iota(jnp.int32, (lanes, lanes), 1)
        ).astype(bf16)
        mask_ref[...] = dot(chosen.astype(bf16), eye, ((0,), (0,))).astype(bf16)
        for copy in copies:
            copy.wait()

    hbm, vmem = pl.BlockSpec(memory_space=pltpu.HBM), pl.BlockSpec(memory_space=pltpu.VMEM)
    return pl.pallas_call(
        kernel,
        out_shape=(
            pltpu.VMEM(shape, bf16),
            pltpu.VMEM((seqs, LANES), f32),
            pltpu.VMEM((seqs, lanes), bf16),
            *[pltpu.VMEM(x.shape, x.dtype) for x in others],
        ),
        in_specs=[hbm] * (count + extra + 2),
        out_specs=(vmem,) * (3 + extra),
        scratch_shapes=[
            pltpu.VMEM(tokens.shape, tokens.dtype),
            pltpu.VMEM(routes.shape, routes.dtype),
            pltpu.SemaphoreType.DMA((count + extra + 2,)),
        ],
        compiler_params=pltpu.CompilerParams(vmem_limit_bytes=4 * 1024 * 1024),
        name="pack",
    )(*[pltpu.with_memory_space_constraint(a, pltpu.HBM) for a in (tokens, routes, *others, *arrays)])


def whole(shape):
    return pl.BlockSpec(shape, lambda *_: tuple(0 for _ in shape))


def project(rows, weights, skip=0):
    block, width = weights[0].shape
    shape = (rows.shape[0], width - skip)

    def kernel(rows_ref, *refs):
        total = None
        for i, weight in enumerate(refs[:-1]):
            piece = dot(rows_ref[:, i * block : (i + 1) * block], weight[:, skip:])
            total = piece if total is None else total + piece
        refs[-1][...] = total.astype(bf16)

    return pl.pallas_call(
        kernel,
        out_shape=jax.ShapeDtypeStruct(shape, bf16),
        in_specs=[whole(rows.shape)] + [whole(w.shape) for w in weights],
        out_specs=whole(shape),
        grid=(1,),
        compiler_params=pltpu.CompilerParams(vmem_limit_bytes=8 * 1024 * 1024),
        name="project",
    )(rows, *weights)


def out_kernel(*refs, count, width, extra):
    messages, weights, out_ref = refs[:count], refs[count:-1], refs[-1]
    rows = jnp.concatenate([m[:, :width] for m in messages], axis=0)
    pieces = [dot(rows, weight[:, :width], ((1,), (1,))).astype(bf16) for weight in weights]
    pieces.append(jnp.concatenate([m[:, width : width + extra] for m in messages], axis=0))
    out_ref[...] = jnp.concatenate(pieces, axis=1)


def out_project(messages, weights, width, extra):
    rows = sum(m.shape[0] for m in messages)
    shape = (rows, sum(w.shape[0] for w in weights) + extra)

    def kernel(*refs):
        out_kernel(*refs, count=len(messages), width=width, extra=extra)

    return pl.pallas_call(
        kernel,
        out_shape=jax.ShapeDtypeStruct(shape, bf16),
        in_specs=[whole(m.shape) for m in messages] + [whole(w.shape) for w in weights],
        out_specs=whole(shape),
        grid=(1,),
        compiler_params=pltpu.CompilerParams(vmem_limit_bytes=8 * 1024 * 1024),
        name="out_project",
    )(*messages, *weights)


def experts_kernel(place, rows_ref, gain_ref, router_ref, *refs, model, experts, groups, cols, seqs):
    gates, ups, downs = refs[:groups], refs[groups : 2 * groups], refs[2 * groups : 3 * groups]
    shared = refs[3 * groups : -3]
    keep_ref, send_ref, total_ref = refs[-3:]
    data = rows_ref[:, :model].astype(f32)
    factor = lax.rsqrt(jnp.sum(data * data, axis=-1, keepdims=True) * (1.0 / model) + epsilon)
    normed = (data * factor * gain_ref[...].astype(f32)).astype(bf16)
    mask = rows_ref[:, model:].astype(f32)[:, :experts]
    prob = jax.nn.sigmoid(dot(normed, router_ref[...], ((1,), (1,)))) * mask
    weight = routed_scale * prob / jnp.sum(prob, axis=-1, keepdims=True)
    lane = lax.broadcasted_iota(jnp.int32, weight.shape, 1)
    total = None
    for g in range(groups):
        for e in range(gates[g].shape[0]):
            expert = place[g] * gates[g].shape[0] + e
            mine = jnp.sum(jnp.where(lane == expert, weight, 0.0), axis=-1, keepdims=True)
            gate = dot(normed, gates[g][e])
            up = dot(normed, ups[g][e])
            hidden = (gate / (1.0 + jnp.exp(-gate)) * up).astype(bf16)
            piece = dot(hidden, downs[g][e]) * mine
            total = piece if total is None else total + piece
    total_ref[...] = total
    if shared:
        gate = dot(normed[:seqs], shared[0][...])
        up = dot(normed[:seqs], shared[1][...])
        hidden = (gate / (1.0 + jnp.exp(-gate)) * up).astype(bf16)
        total_ref[:seqs] = total[:seqs] + dot(hidden, shared[2][...])
    for target, i in ((send_ref, 1), (keep_ref, 0)):
        window = pl.ds(pl.multiple_of(place[groups + i], LANES), cols)
        target[...] = total_ref[:, window].astype(target.dtype)


def run_experts(rows, gain, router, gates, ups, downs, place, cols, seqs, shared=()):
    count = rows.shape[0]
    model = gates[0].shape[1]

    def kernel(*refs):
        experts_kernel(*refs, model=model, experts=router.shape[0], groups=len(gates), cols=cols, seqs=seqs)

    return pl.pallas_call(
        kernel,
        out_shape=(jax.ShapeDtypeStruct((count, cols), f32), jax.ShapeDtypeStruct((count, cols), bf16)),
        grid_spec=pltpu.PrefetchScalarGridSpec(
            num_scalar_prefetch=1,
            grid=(1,),
            in_specs=[whole(rows.shape), whole((1, model)), whole(router.shape)]
            + [pl.BlockSpec(memory_space=pltpu.VMEM)] * (3 * len(gates) + len(shared)),
            out_specs=(whole((count, cols)), whole((count, cols))),
            scratch_shapes=[pltpu.VMEM((count, model), f32)],
        ),
        compiler_params=pltpu.CompilerParams(vmem_limit_bytes=12 * 1024 * 1024),
        name="routed_experts",
    )(
        place,
        rows,
        gain,
        router,
        *[pltpu.with_memory_space_constraint(w, pltpu.VMEM) for w in (*gates, *ups, *downs, *shared)],
    )


def make_body(n_ep, n_tp):
    inner = 1 << ((n_ep.bit_length() - 1) // 2)
    outer = n_ep // inner
    masks = [1 << i for i in reversed(range(inner.bit_length() - 1))]

    def swap(value, mask):
        return lax.ppermute(value, "ep", [(i, i ^ mask) for i in range(n_ep)])

    def outer_swap(value, k):
        return swap(value, k * inner)

    def outer_exchange(messages):
        got = {}
        for k in reversed(range(1, outer)):
            got[k] = outer_swap(messages[k], k)
        return [messages[0]] + [got[k] for k in range(1, outer)]

    def tp_swap(value):
        return lax.ppermute(value, "tp", [(i, (i + 1) % n_tp) for i in range(n_tp)])

    def gather(value, over):
        pieces, order = [value], [0]
        for m in over:
            more = []
            for piece in pieces:
                more.append(swap(piece, m))
            pieces = pieces + more
            order = order + [o ^ m for o in order]
        return pieces, order

    def reverse_bits(value):
        result, width = jnp.uint32(0), inner
        while width > 1:
            result = (result << 1) | (value & 1)
            value = value >> 1
            width = width // 2
        return result

    def cut(value, start, size):
        return lax.dynamic_slice(value, (jnp.uint32(0), start), (value.shape[0], size))

    def body(
        tokens,
        attn_gain,
        query_weight,
        key_weight,
        value_weight,
        out_weight,
        head_gain,
        past_keys,
        past_values,
        break_offset,
        cache_lengths,
        ffn_gain,
        router_weight,
        expert_routes,
        expert_gate,
        expert_up,
        expert_down,
        shared_gate,
        shared_up,
        shared_down,
    ):
        seqs, model = tokens.shape
        experts = router_weight.shape[1]
        block = query_weight.shape[0]
        plane = block * inner
        cols = model // n_tp
        key_cols = key_weight.shape[1]
        heads_width = out_weight.shape[1]
        pad = -experts % LANES

        me = lax.axis_index("ep").astype(jnp.uint32)
        my_tp = lax.axis_index("tp").astype(jnp.uint32)
        my_inner = me & (inner - 1)
        my_outer = me >> (inner.bit_length() - 1)
        marks = [my_outer ^ k for k in range(outer)]
        starts = [m * plane for m in marks]
        blocks_at = [(my_inner ^ o) * block for o in range(inner)]
        back_at = [reverse_bits(my_inner ^ o) * block for o in range(inner)]
        own_start, other_start = my_tp * cols, ((my_tp + 1) & (n_tp - 1)) * cols
        row_starts = [m * (outer * seqs) for m in marks]
        place = jnp.stack([me, me ^ 1, own_start, other_start]).astype(jnp.int32)
        held = (tokens, starts, row_starts, blocks_at, back_at, own_start, place)
        held = lax.optimization_barrier(held)
        tokens, starts, row_starts, blocks_at, back_at, own_start, place = held

        query_pieces, order = gather(query_weight, masks)
        got = outer_exchange([cut(tokens, start, plane) for start in starts])
        group_tokens = jnp.concatenate(got, axis=0)

        def by_order(value):
            return jnp.concatenate([cut(value, blocks_at[o], block) for o in order], axis=1)

        gain_plane = cut(attn_gain.reshape(1, model), starts[0], plane)
        ordered = by_order(group_tokens)
        gained = (ordered.astype(f32) * by_order(gain_plane).astype(f32)).astype(bf16)
        query_pieces[0] = load_weights([query_weight])[0]
        query_part = project(gained, query_pieces)
        query_part, routes, gains, late_tokens, packs = lax.optimization_barrier(
            (query_part, expert_routes, (head_gain, ffn_gain), tokens, (out_weight, key_weight, value_weight))
        )
        query_got = outer_exchange([query_part[k * seqs : (k + 1) * seqs] for k in range(outer)])
        ffn_row = gains[1].reshape(1, -1)
        packed, factor, routed_mask, offsets, gain_row, lengths = pack(
            packs, (break_offset, gains[0], cache_lengths), late_tokens, routes.T, experts + pad
        )
        factor = factor[:, :1]
        late_pieces, _ = gather(packed, masks[:-1])
        queries = (sum(part.astype(f32) for part in query_got) * factor).astype(bf16).astype(f32)

        held = lax.optimization_barrier((query_part, expert_gate, expert_up, expert_down))
        query_part, expert_gate, expert_up, expert_down = held
        gates, ups, downs = [[w, swap(w, 1)] for w in (expert_gate, expert_up, expert_down)]
        scaled = attend(
            queries, past_keys, past_values, offsets, lengths, gain_row, routed_mask
        )
        held = lax.optimization_barrier((scaled, gates, ups, downs, late_pieces))
        scaled, gates, ups, downs, late_pieces = held
        late_pieces = late_pieces + [swap(p, masks[-1]) for p in late_pieces]
        arrived = outer_exchange([scaled] * outer)
        group_mask = jnp.concatenate([m[:, heads_width + LANES :] for m in arrived], axis=0)
        own_part = out_project(arrived, late_pieces, heads_width, LANES)
        own_part, *shared = lax.optimization_barrier((own_part, shared_gate, shared_up, shared_down))
        shared = load_weights(shared)
        other_part = tp_swap(own_part)
        both = own_part.astype(f32) + other_part.astype(f32)
        square_total = jnp.sum(both[:, plane:], axis=1, keepdims=True)
        attention = both[:, :plane] * lax.rsqrt(square_total / (heads_width * n_tp) + epsilon)
        residual_part = (ordered.astype(f32) + attention).astype(bf16)

        residual_plane = jnp.concatenate([cut(residual_part, back_at[o], block) for o in range(inner)], axis=1)
        held = lax.optimization_barrier((residual_plane, gates, ups, downs, gained, shared))
        residual_plane, gates, ups, downs, gained, shared = held
        loaded = load_weights((*gates, *ups, *downs))
        gates, ups, downs = loaded[:2], loaded[2:4], loaded[4:]
        peers = outer_exchange([residual_plane] * outer)
        stacked = []
        for k in range(outer):
            stacked += [peers[k][(j ^ k) * seqs : (j ^ k) * seqs + seqs] for j in range(outer)]
        stacked = jnp.concatenate(stacked, axis=0)
        group_rows = jnp.concatenate(
            [lax.dynamic_slice(stacked, (row_starts[p], jnp.uint32(0)), (outer * seqs, plane)) for p in range(outer)]
            + [group_mask],
            axis=1,
        )
        group_rows, gates, ups, downs = lax.optimization_barrier((group_rows, gates, ups, downs))
        row_pieces, _ = gather(group_rows, masks[:-1])

        rest_part = project(gained, late_pieces, heads_width)
        rest_got = outer_exchange([rest_part[k * seqs : (k + 1) * seqs] for k in range(outer)])
        fresh = (sum(part.astype(f32) for part in rest_got) * factor).astype(bf16)
        own_rows = group_rows[:seqs, :model]

        router = router_weight.T
        results = []
        for i, piece in enumerate(row_pieces):
            extra = shared if i == 0 else ()
            results.append(run_experts(piece, ffn_row, router, gates, ups, downs, place, cols, seqs, extra))
        sums = []
        for pair in results:
            sums.append(pair[0] + tp_swap(pair[1]).astype(f32))
        for m in reversed(masks[:-1]):
            half = len(sums) // 2
            back = [swap(v.astype(bf16), m) for v in sums[half:]]
            sums = [a + b.astype(f32) for a, b in zip(sums[:half], back)]
        value = sums[0]
        value_out = value.astype(bf16)
        parts = outer_exchange([value_out[k * seqs : (k + 1) * seqs] for k in range(outer)])
        total = value[:seqs] + sum(part.astype(f32) for part in parts[1:])
        mixed = (cut(own_rows, own_start, cols).astype(f32) + total).astype(bf16)
        return mixed, fresh[:, :key_cols], fresh[:, key_cols:]

    return body


def solution(mesh):
    placed = (
        P("ep", None),
        P(),
        P("ep", "tp"),
        P("ep", "tp"),
        P("ep", "tp"),
        P("ep", "tp"),
        P("tp"),
        P("ep", None, "tp", None),
        P("ep", None, "tp", None),
        P("ep", "tp", None),
        P("ep"),
        P(),
        P(),
        P("ep", None),
        P("ep", None, "tp"),
        P("ep", None, "tp"),
        P("ep", "tp", None),
        P(None, "tp"),
        P(None, "tp"),
        P("tp", None),
    )
    n_ep = mesh.shape["ep"]
    step = make_body(n_ep, mesh.shape["tp"])

    return jax.shard_map(
        step,
        mesh=mesh,
        in_specs=placed,
        out_specs=(P("ep", "tp"), P("ep", "tp"), P("ep", "tp")),
        check_vma=False,
    )
```
